256 devices in a mesh: sp: 64 (over z, x, core), tp: 4 (over y).
Axes of the slice: x: 4, y: 4, z: 8, core: 2. Of those that a mesh axis runs over, the one named last changes fastest.
Arguments:
- queries: bfloat16 [8192, 2048], P('sp', 'tp'), may hold values from -6 to 6
- key_rows: bfloat16 [8192, 2048], P('sp', 'tp'), may hold values from -6 to 6
- value_rows: bfloat16 [8192, 2048], P('sp', 'tp'), may hold values from -6 to 6
- gate_input: bfloat16 [8192, 2048], P('sp', 'tp'), may hold values from -6 to 6
- log_decay: float32 [8192, 16], P('sp', 'tp'), may hold values from -0.6 to 0, as said below
- head_gain: float32 [2048], P('tp'), may hold values from 0.1 to 1.9
- out_weight: bfloat16 [2048, 2048], P('tp'), may hold values from -0.125 to 0.125
- residual: bfloat16 [8192, 2048], P('sp'), may hold values from -6 to 6
- mlp_gain: float32 [2048], replicated, may hold values from 0.1 to 1.9
- gate_weight: bfloat16 [2048, 5632], P('sp', 'tp'), may hold values from -0.125 to 0.125
- up_weight: bfloat16 [2048, 5632], P('sp', 'tp'), may hold values from -0.125 to 0.125
- down_weight: bfloat16 [5632, 2048], P('tp', 'sp'), may hold values from -0.078125 to 0.078125
Outputs:
- layer_out: bfloat16 [8192, 2048], P(('sp', 'tp'))
The draws below stay inside these ranges and needn't reach their ends.
Inputs may be any that keep to these rules, and one draw needn't show every extreme that they name: log_decay holds the logarithm of a decay factor of each head at each position.
All inputs are finite; a program needn't handle non-finite values.
Results may differ from the reference program's by a relative error of at most 0.017.
Values may be sent and summed in bfloat16 or wider, within the bound.
A program may use at most 128 MiB of HBM per device.

```python
import math
import jax
import jax.numpy as jnp
from jax import lax

D = 2048
RETENTION_HEADS = 16
HD = 128
FF = 5632
BLOCK = 128
TOK_DEV = 128
SEQUENCE_TOKENS = 8192
N_TP = 4


def draw_log_decay(key, part):
    key_collection = jax.random.split(jax.random.fold_in(key, 11), 5)
    slow_kind = jax.random.randint(key_collection[0], (RETENTION_HEADS,), 0, 10) < 5
    fast_length = jnp.exp(jax.random.uniform(key_collection[1], (RETENTION_HEADS,), jnp.float32, math.log(30.0), math.log(100.0)))
    fast_rate = -1.0 / fast_length
    device_blocks = SEQUENCE_TOKENS // TOK_DEV
    factor = jnp.exp(jax.random.uniform(key_collection[2], (device_blocks, RETENTION_HEADS), jnp.float32, math.log(0.4), math.log(1.6)))
    slow_rate = jnp.repeat(factor, TOK_DEV, axis=0) * (-0.4 / SEQUENCE_TOKENS)
    spike_positions = jax.random.randint(key_collection[3], (3, RETENTION_HEADS), 0, SEQUENCE_TOKENS)
    spike_length = jnp.log(jax.random.uniform(key_collection[4], (3, RETENTION_HEADS), jnp.float32, 0.6, 0.8))
    token_spots = jnp.arange(SEQUENCE_TOKENS, dtype=jnp.int32)[:, None, None]
    spike_rows = jnp.sum(jnp.where(token_spots == spike_positions[None], spike_length[None], 0.0), axis=1)
    constant_level = jnp.where(slow_kind[None, :], slow_rate, fast_rate[None, :])
    return (constant_level + spike_rows).astype(jnp.float32)


def levels(rng, shape, cuts, smallest, high):
    level = 1.0
    for dim, parts in cuts:
        heights = jax.random.uniform(jax.random.fold_in(jax.random.fold_in(rng, 6), dim), (parts,), jnp.float32, smallest / len(cuts), high / len(cuts))
        level = level * jnp.repeat(jnp.exp(heights), shape[dim] // parts).reshape((-1,) + (1,) * (len(shape) - 1 - dim))
    return level


def gaussian(own_key, shape, scale, reach, pieces=(), kind=jnp.bfloat16):
    drawn = scale * jax.random.normal(own_key, shape, jnp.float32)
    if pieces:
        drawn = drawn * levels(own_key, shape, pieces, -0.22, 0.18)
    return jnp.clip(drawn, -reach, reach).astype(kind)


def setup_inputs(seed: int = 0) -> dict:
    streams_of = jax.random.split(jax.random.key(seed), 13)
    return {
        "queries": gaussian(streams_of[0], (SEQUENCE_TOKENS, RETENTION_HEADS * HD), 1.0, 6.0, ((0, 64), (1, 4))),
        "key_rows": gaussian(streams_of[1], (SEQUENCE_TOKENS, RETENTION_HEADS * HD), 1.0, 6.0, ((0, 64), (1, 4))),
        "value_rows": gaussian(streams_of[2], (SEQUENCE_TOKENS, RETENTION_HEADS * HD), 1.0, 6.0, ((0, 64), (1, 4))),
        "gate_input": gaussian(streams_of[3], (SEQUENCE_TOKENS, RETENTION_HEADS * HD), 1.0, 6.0, ((0, 64), (1, 4))),
        "log_decay": draw_log_decay(jax.random.fold_in(streams_of[12], 71), 0),
        "head_gain": jnp.clip(1.0 + 0.18 * jax.random.normal(streams_of[5], (RETENTION_HEADS * HD,), jnp.float32), 0.1, 1.9),
        "out_weight": gaussian(streams_of[6], (RETENTION_HEADS * HD, D), (RETENTION_HEADS * HD) ** -0.5, 0.125, ((0, 4),)),
        "residual": gaussian(streams_of[7], (SEQUENCE_TOKENS, D), 1.0, 6.0, ((0, 64),)),
        "mlp_gain": jnp.clip(1.0 + 0.18 * jax.random.normal(streams_of[8], (D,), jnp.float32), 0.1, 1.9),
        "gate_weight": gaussian(streams_of[9], (D, FF), D ** -0.5, 0.125, ((0, 64), (1, 4))),
        "up_weight": gaussian(streams_of[10], (D, FF), D ** -0.5, 0.125, ((0, 64), (1, 4))),
        "down_weight": gaussian(streams_of[11], (FF, D), FF ** -0.5, 0.078125, ((0, 4), (1, 64))),
    }


EPS = 1e-06

def rotate(values_in, positions):
    half = values_in.shape[-1] // 2
    freq = 10000.0 ** (-jnp.linspace(0.0, 1.0, half, dtype=jnp.float32))
    angles = positions * freq
    angles = jnp.concatenate([angles, angles], axis=-1)
    first = values_in[..., :half]
    second = values_in[..., half:]
    turned = jnp.concatenate([-second, first], axis=-1)
    return values_in * jnp.cos(angles) + turned * jnp.sin(angles)

def row_norm(stream, gain):
    return stream * lax.rsqrt(lax.optimization_barrier(jnp.mean(stream * stream, axis=-1, keepdims=True)) + EPS) * gain

def retain_head(inputs):
    query_head, key_head, value_head, decay_head, gain_head = inputs
    length = query_head.shape[0]
    positions = jnp.arange(length, dtype=jnp.float32)[:, None]
    q_rot = rotate(query_head.astype(jnp.float32), positions).astype(jnp.bfloat16)
    k_rot = (rotate(key_head.astype(jnp.float32), positions) * HD ** (-0.5)).astype(jnp.bfloat16)
    blocks = length // BLOCK
    q_blocks = q_rot.reshape(blocks, BLOCK, HD).astype(jnp.float32)
    k_blocks = k_rot.reshape(blocks, BLOCK, HD).astype(jnp.float32)
    v_blocks = value_head.reshape(blocks, BLOCK, HD).astype(jnp.float32)
    cumul = jnp.cumsum(decay_head.reshape(blocks, BLOCK), axis=1)
    lower = jnp.tril(jnp.ones((BLOCK, BLOCK), dtype=bool))
    spread = cumul[:, :, None] - cumul[:, None, :]
    weight = jnp.where(lower, jnp.exp(jnp.where(lower, spread, 0.0)), 0.0)
    scores = jnp.einsum('ntd,nsd->nts', q_blocks, k_blocks)
    probs = (scores * weight).astype(jnp.bfloat16).astype(jnp.float32)
    inner = jnp.einsum('nts,nse->nte', probs, v_blocks)
    k_weighted = (k_blocks * jnp.exp(cumul[:, -1:] - cumul)[:, :, None]).astype(jnp.bfloat16).astype(jnp.float32)
    contrib = jnp.einsum('nsd,nse->nde', k_weighted, v_blocks)
    totals = jnp.exp(cumul[:, -1])

    def advance(state, items):
        factor, update = items
        return (state * factor + update, state)
    _, before = lax.scan(advance, jnp.zeros((HD, HD), jnp.float32), (totals, contrib))
    cross = jnp.einsum('ntd,nde->nte', q_blocks, before, precision=lax.Precision.HIGHEST)
    cross = cross * jnp.exp(cumul)[:, :, None]
    result = (inner + cross).reshape(length, HD)
    return row_norm(result, gain_head)

def reference(queries, key_rows, value_rows, gate_input, log_decay, head_gain, out_weight, residual, mlp_gain, gate_weight, up_weight, down_weight):

    def by_head(array):
        return array.reshape(SEQUENCE_TOKENS, RETENTION_HEADS, HD).transpose(1, 0, 2)
    heads_out = lax.map(retain_head, (by_head(queries), by_head(key_rows), by_head(value_rows), log_decay.T, head_gain.reshape(RETENTION_HEADS, HD)))
    joined = heads_out.transpose(1, 0, 2).reshape(SEQUENCE_TOKENS, RETENTION_HEADS * HD)
    gate_act = jax.nn.silu(gate_input.astype(jnp.float32))
    retained = (joined * gate_act).astype(jnp.bfloat16)
    width = RETENTION_HEADS * HD // N_TP
    hidden_width = FF // N_TP

    def layer_block(items):
        ret_rows, res_rows = items
        mixed = jnp.zeros((TOK_DEV, D), jnp.float32)
        for group_idx in range(N_TP):
            part = jnp.dot(ret_rows[:, group_idx * width:(group_idx + 1) * width], out_weight[group_idx * width:(group_idx + 1) * width], preferred_element_type=jnp.float32)
            part = lax.optimization_barrier(part.astype(jnp.bfloat16))
            mixed = mixed + part.astype(jnp.float32)
        middle = (res_rows.astype(jnp.float32) + mixed).astype(jnp.bfloat16)
        normed = row_norm(middle.astype(jnp.float32), mlp_gain).astype(jnp.bfloat16)
        gate = jnp.dot(normed, gate_weight, preferred_element_type=jnp.float32)
        upvals = jnp.dot(normed, up_weight, preferred_element_type=jnp.float32)
        hidden = (jax.nn.silu(gate) * upvals).astype(jnp.bfloat16)
        ffn = jnp.zeros((TOK_DEV, D), jnp.float32)
        for group_idx in range(N_TP):
            part = jnp.dot(hidden[:, group_idx * hidden_width:(group_idx + 1) * hidden_width], down_weight[group_idx * hidden_width:(group_idx + 1) * hidden_width], preferred_element_type=jnp.float32)
            part = lax.optimization_barrier(part.astype(jnp.bfloat16))
            ffn = ffn + part.astype(jnp.float32)
        return (middle.astype(jnp.float32) + ffn).astype(jnp.bfloat16)
    outcome = lax.map(layer_block, (retained.reshape(-1, TOK_DEV, RETENTION_HEADS * HD), residual.reshape(-1, TOK_DEV, D)))
    return outcome.reshape(SEQUENCE_TOKENS, D)
```

```python
import heapq

import jax
import jax.numpy as jnp
from jax import lax
from jax.experimental import pallas as pl
from jax.experimental.pallas import tpu as pltpu
from jax.sharding import Mesh
from jax.sharding import PartitionSpec as P

BF = jnp.bfloat16
F32 = jnp.float32
MESH = pl.DeviceIdType.MESH
HIGH = lax.Precision.HIGHEST
EPS = 1e-06

NZ, NX, NC, NT = 8, 4, 2, 4
SP = ("z", "x", "c")
TOK = 128
HD = 128
HEADS = 4
D = 2048
FF = 1408
ROWS = 32
QT = TOK // NT
GATE, UP, DOWN = 0, 1, 2

PIECE_US = 1.95
HOP_US = 1.9


def forward_reach(a, dx):
    if a == UP:
        return 4 if dx % 2 == 0 else 3
    return 4 if a == GATE else 3


def onward(a, dz, dx):
    links = []
    reach = forward_reach(a, dx)
    if dz == 0:
        along_z = ["z+", "z-"]
    elif dz <= reach:
        along_z = ["z+"] if dz < reach else []
    else:
        along_z = ["z-"] if NZ - dz < NZ - 1 - reach else []
    plus = True if a == UP else dz % 2 == 0
    if dx == 0:
        along_x = ["x+", "x-"]
    elif dx == 1:
        along_x = ["x+"] if plus else []
    elif dx == 3:
        along_x = [] if plus else ["x-"]
    else:
        along_x = []
    if a == UP:
        links += along_z
        if dz == 0:
            links += along_x
    else:
        if dx == 0:
            links += along_z
        links += along_x
    return links


def arrives_as(link, key):
    a, dz, dx = key
    if link == "z+":
        return (a, (dz + 1) % NZ, dx)
    if link == "z-":
        return (a, (dz - 1) % NZ, dx)
    if link == "x+":
        return (a, dz, (dx + 1) % NX)
    return (a, dz, (dx - 1) % NX)


def exchange_plan():
    rank = {GATE: 0, UP: 0, DOWN: 1}
    pending = {l: [] for l in ("z+", "z-", "x+", "x-")}
    free = dict.fromkeys(pending, 0.0)
    arrivals = []
    ops = []
    count = 0

    def ready(now, key):
        nonlocal count
        for link in onward(*key):
            count += 1
            heapq.heappush(pending[link], (rank[key[0]], now, count, key))

    for a in (GATE, UP, DOWN):
        ready(0.0, (a, 0, 0))
    now = 0.0
    while True:
        for link, queue in pending.items():
            if queue and free[link] <= now:
                _, since, _, key = heapq.heappop(queue)
                free[link] = now + PIECE_US
                ops.append((max(since, now - PIECE_US), 1, "send", link, key))
                count += 1
                heapq.heappush(arrivals, (now + PIECE_US + HOP_US, count, arrives_as(link, key)))
        times = [t for l, t in free.items() if pending[l] and t > now]
        if arrivals:
            times.append(arrivals[0][0])
        if not times:
            break
        now = min(times)
        while arrivals and arrivals[0][0] <= now:
            _, _, key = heapq.heappop(arrivals)
            ops.append((now, 0, "recv", None, key))
            ready(now, key)
    ops.sort(key=lambda op: (op[0], op[1]))
    return ops


PLAN = exchange_plan()
SENT = {a: sum(1 for op in PLAN if op[2] == "send" and op[4][0] == a) for a in (GATE, UP, DOWN)}

T_CONTRIB, T_GROUP, T_ALONG, T_BACK, T_SUM1, T_GATHER = 2.5, 8.0, 14.0, 19.0, 30.0, 37.0


def head_cols(h):
    return slice(h * HD, (h + 1) * HD)


def split_log(total):
    hi = total.astype(BF).astype(F32)
    rest = total - hi
    mid = rest.astype(BF).astype(F32)
    low = rest - mid
    i = lax.broadcasted_iota(jnp.int32, (16, HD), 0)
    return jnp.where(i == 0, hi, jnp.where(i == 1, mid, low)).astype(BF)


def join_log(tile):
    t = tile.astype(F32)
    return t[0:1] + t[1:2] + t[2:3]


def silu(v):
    return v * (1.0 / (1.0 + jnp.exp(-v)))


def kernel(
    q_ref, k_ref, v_ref, gi_ref, ld_ref, cos_ref, sin_ref, hg_ref, ow_ref, res_ref, mg_ref,
    gw_ref, uw_ref, dw_ref,
    out_ref,
    w, ldp, qrot, inner, ret, stout, stin, pre, zout, zin, bout, bin_, po, rs1, nfull, mid,
    gacc, uacc, hid, fo, rs2,
    w_recv, w_send, d_recv, d_send,
    g_recv, g_send, z_recv, z_send, b_recv, b_send, r_recv, r_send, n_recv, n_send, f_recv, f_send,
):
    z, x, c, t = lax.axis_index("z"), lax.axis_index("x"), lax.axis_index("c"), lax.axis_index("tp")
    pos = x * NC + c

    def group_peer(r):
        p = lax.rem(pos + r, NX * NC)
        return p, (z, lax.div(p, NC), lax.rem(p, NC), t)

    def z_peer(r):
        return (lax.rem(z + r, NZ), x, c, t)

    def tp_peer(r):
        j = lax.rem(t + r, NT)
        return j, (z, x, c, j)

    neighbours = {
        "z+": (lax.rem(z + 1, NZ), x, c, t),
        "z-": (lax.rem(z + NZ - 1, NZ), x, c, t),
        "x+": (z, lax.rem(x + 1, NX), c, t),
        "x-": (z, lax.rem(x + NX - 1, NX), c, t),
    }
    partner = (z, x, 1 - c, t)

    barrier = pltpu.get_barrier_semaphore()
    for r in range(1, NX * NC):
        pl.semaphore_signal(barrier, inc=1, device_id=group_peer(r)[1], device_id_type=MESH)
    for r in range(1, NZ):
        pl.semaphore_signal(barrier, inc=1, device_id=z_peer(r), device_id_type=MESH)
    for r in range(1, NT):
        pl.semaphore_signal(barrier, inc=1, device_id=tp_peer(r)[1], device_id_type=MESH)
    pl.semaphore_wait(barrier, NX * NC - 1 + NZ - 1 + NT - 1)

    own = {GATE: gw_ref, UP: uw_ref, DOWN: dw_ref}

    def rows_of(dz, dx, core):
        sz = lax.rem(z + NZ - dz, NZ)
        sx = lax.rem(x + NX - dx, NX)
        return pl.ds(pl.multiple_of(((sz * NX + sx) * NC + core) * ROWS, ROWS), ROWS)

    def at_home(key):
        a, dz, dx = key
        return w.at[a, rows_of(dz, dx, c), :]

    def source(key):
        return own[key[0]] if key[1:] == (0, 0) else at_home(key)

    def hop(link, key):
        a, dz, dx = arrives_as(link, key)
        return pltpu.make_async_remote_copy(
            src_ref=source(key), dst_ref=at_home(key), send_sem=w_send.at[key[0]],
            recv_sem=w_recv.at[a, dz, dx], device_id=neighbours[link], device_id_type=MESH,
        )

    def across(key):
        a, dz, dx = key
        return pltpu.make_async_remote_copy(
            src_ref=source(key), dst_ref=at_home(key), send_sem=d_send.at[a, dz],
            recv_sem=d_recv.at[a, dz], device_id=partner, device_id_type=MESH,
        )

    cursor = [0]

    def step(op):
        _, _, kind, link, key = op
        if kind == "send":
            hop(link, key).start()
        else:
            a, dz, dx = key
            pltpu.make_async_remote_copy(
                src_ref=at_home(key), dst_ref=at_home(key), send_sem=w_send.at[a],
                recv_sem=w_recv.at[a, dz, dx], device_id=partner, device_id_type=MESH,
            ).wait_recv()
            across(key).start()

    def run_until(time):
        while cursor[0] < len(PLAN) and PLAN[cursor[0]][0] <= time:
            step(PLAN[cursor[0]])
            cursor[0] += 1

    def run_until_received(wanted):
        last = max(i for i, op in enumerate(PLAN) if op[2] == "recv" and wanted(op[4]))
        while cursor[0] <= last:
            step(PLAN[cursor[0]])
            cursor[0] += 1

    def wait_across(a, dz):
        whole = w.at[a, pl.ds(0, NX * ROWS), :]
        pltpu.make_async_remote_copy(
            src_ref=whole, dst_ref=whole, send_sem=d_send.at[a, dz],
            recv_sem=d_recv.at[a, dz], device_id=partner, device_id_type=MESH,
        ).wait_recv()

    run_until(0.0)
    for a in (GATE, UP, DOWN):
        across((a, 0, 0)).start()

    ldp[...] = jnp.zeros((TOK, HD), F32)
    ldp[:, 0:HEADS] = ld_ref[...]
    ti = lax.broadcasted_iota(jnp.int32, (TOK, TOK), 0)
    si = lax.broadcasted_iota(jnp.int32, (TOK, TOK), 1)
    lower = si <= ti
    cum = jnp.dot(lower.astype(F32), ldp[...], precision=HIGH, preferred_element_type=F32)
    cum_t = cum.T
    cosv, sinv = cos_ref[...], sin_ref[...]
    krots = []
    for h in range(HEADS):
        kf = k_ref[:, head_cols(h)].astype(F32)
        krot = ((kf * cosv + pltpu.roll(kf, HD // 2, 1) * sinv) * HD ** (-0.5)).astype(BF)
        krots.append(krot)
        col = cum[:, h : h + 1]
        last = cum[TOK - 1 : TOK, h : h + 1]
        kw = (krot.astype(F32) * jnp.exp(last - col)).astype(BF)
        contrib = jnp.dot(kw.T, v_ref[:, head_cols(h)], preferred_element_type=F32)
        logs = split_log(jnp.broadcast_to(last, (1, HD)))
        for half in range(2):
            stout[2 * h + half, 0:64, :] = contrib[64 * half : 64 * half + 64].astype(BF)
            stout[2 * h + half, 64:80, :] = logs
    for a in (GATE, UP, DOWN):
        w[a, rows_of(0, 0, c), :] = own[a][...]
    run_until(T_CONTRIB)

    def group_copy(r):
        p, peer = group_peer(r)
        return pltpu.make_async_remote_copy(
            src_ref=stout.at[p], dst_ref=stin.at[pos], send_sem=g_send.at[r],
            recv_sem=g_recv.at[r], device_id=peer, device_id_type=MESH,
        )

    for r in range(1, NX * NC):
        group_copy(r).start()
    stin[pos] = stout[pos]

    for h in range(HEADS):
        qf = q_ref[:, head_cols(h)].astype(F32)
        qr = (qf * cosv + pltpu.roll(qf, HD // 2, 1) * sinv).astype(BF)
        qrot[:, head_cols(h)] = qr
        spread = cum[:, h : h + 1] - cum_t[h : h + 1, :]
        weight = jnp.where(lower, jnp.exp(jnp.where(lower, spread, 0.0)), 0.0)
        scores = lax.dot_general(qr, krots[h], (((1,), (1,)), ((), ())), preferred_element_type=F32)
        probs = (scores * weight).astype(BF)
        inner[:, head_cols(h)] = jnp.dot(probs, v_ref[:, head_cols(h)], preferred_element_type=F32)
    run_until(T_GROUP)

    for r in range(1, NX * NC):
        group_copy(r).wait_recv()
    run = jnp.zeros((64, HD), F32)
    sofar = jnp.zeros((1, HD), F32)
    reach = []
    for p in range(NX * NC):
        pre[p] = run
        reach.append(sofar)
        log = join_log(stin[p, 64:80, :])
        run = run * jnp.exp(log) + stin[p, 0:64, :].astype(F32)
        sofar = sofar + log
    zout[0:64, :] = run.astype(BF)
    zout[64:80, :] = split_log(sofar)

    def z_copy(r):
        return pltpu.make_async_remote_copy(
            src_ref=zout, dst_ref=zin.at[z], send_sem=z_send.at[r],
            recv_sem=z_recv.at[r], device_id=z_peer(r), device_id_type=MESH,
        )

    for r in range(1, NZ):
        z_copy(r).start()
    zin[z] = zout[...]
    run_until(T_ALONG)
    for r in range(1, NZ):
        z_copy(r).wait_recv()
    came = jnp.zeros((64, HD), F32)
    for s in range(NZ):
        log = join_log(zin[s, 64:80, :])
        came = jnp.where(s < z, came * jnp.exp(log) + zin[s, 0:64, :].astype(F32), came)
    for p in range(NX * NC):
        bout[p] = (pre[p] + jnp.exp(reach[p]) * came).astype(BF)

    def back_copy(r):
        p, peer = group_peer(r)
        return pltpu.make_async_remote_copy(
            src_ref=bout.at[p], dst_ref=bin_.at[pos], send_sem=b_send.at[r],
            recv_sem=b_recv.at[r], device_id=peer, device_id_type=MESH,
        )

    for r in range(1, NX * NC):
        back_copy(r).start()
    bin_[pos] = bout[pos]
    run_until(T_BACK)
    for r in range(1, NX * NC):
        back_copy(r).wait_recv()

    for h in range(HEADS):
        before = bin_[2 * h : 2 * h + 2].reshape(HD, HD)
        cross = jnp.dot(qrot[:, head_cols(h)], before, preferred_element_type=F32)
        res = inner[:, head_cols(h)] + cross * jnp.exp(cum[:, h : h + 1])
        scale = lax.rsqrt(jnp.mean(res * res, axis=-1, keepdims=True) + EPS)
        gain = hg_ref[:, head_cols(h)]
        ret[:, head_cols(h)] = (
            res * scale * gain * silu(gi_ref[:, head_cols(h)].astype(F32))
        ).astype(BF)
    for n in range(0, D, 512):
        po[:, n : n + 512] = jnp.dot(
            ret[...], ow_ref[:, n : n + 512], preferred_element_type=F32
        ).astype(BF)

    mine = pl.ds(pl.multiple_of(t * QT, QT), QT)

    def sum_copy(r):
        j, peer = tp_peer(r)
        return pltpu.make_async_remote_copy(
            src_ref=po.at[pl.ds(pl.multiple_of(j * QT, QT), QT), :], dst_ref=rs1.at[r - 1],
            send_sem=r_send.at[r], recv_sem=r_recv.at[r], device_id=peer, device_id_type=MESH,
        )

    for r in (2, 1, 3):
        sum_copy(r).start()
    run_until(T_SUM1)
    for r in range(1, NT):
        sum_copy(r).wait_recv()
    mixed = po[mine, :].astype(F32)
    for r in range(NT - 1):
        mixed = mixed + rs1[r].astype(F32)
    middle = (res_ref[...].astype(F32) + mixed).astype(BF).astype(F32)
    mid[...] = middle
    scale = lax.rsqrt(jnp.mean(middle * middle, axis=-1, keepdims=True) + EPS)
    nfull[mine, :] = (middle * scale * mg_ref[...]).astype(BF)

    def norm_copy(r):
        return pltpu.make_async_remote_copy(
            src_ref=nfull.at[mine, :], dst_ref=nfull.at[mine, :],
            send_sem=n_send.at[r], recv_sem=n_recv.at[r], device_id=tp_peer(r)[1],
            device_id_type=MESH,
        )

    def norm_arrived(r):
        rows = nfull.at[pl.ds(pl.multiple_of(lax.rem(t + NT - r, NT) * QT, QT), QT), :]
        pltpu.make_async_remote_copy(
            src_ref=rows, dst_ref=rows, send_sem=n_send.at[r], recv_sem=n_recv.at[r],
            device_id=partner, device_id_type=MESH,
        ).wait_recv()

    for r in (2, 1, 3):
        norm_copy(r).start()
    run_until(T_GATHER)
    for r in range(1, NT):
        norm_arrived(r)

    run_until_received(lambda key: key[0] != DOWN)
    for a in (GATE, UP):
        for dz in range(NZ):
            wait_across(a, dz)
    clock = PLAN[cursor[0] - 1][0]
    for n in range(NZ):
        rows = slice(n * 256, (n + 1) * 256)
        for a, acc in ((GATE, gacc), (UP, uacc)):
            term = jnp.dot(nfull[:, rows], w[a, rows, :], preferred_element_type=F32)
            acc[...] = term if n == 0 else acc[...] + term
        clock += 0.6
        run_until(clock)
    hid[...] = (silu(gacc[...]) * uacc[...]).astype(BF)

    def ffn_copy(r, zc):
        j, peer = tp_peer(r)
        return pltpu.make_async_remote_copy(
            src_ref=fo.at[zc, pl.ds(pl.multiple_of(j * QT, QT), QT), :], dst_ref=rs2.at[r - 1, zc],
            send_sem=f_send.at[r], recv_sem=f_recv.at[r], device_id=peer, device_id_type=MESH,
        )

    last = {}
    for i, op in enumerate(PLAN):
        if op[2] == "recv" and op[4][0] == DOWN:
            last[op[4][1]] = i
    for dz in sorted(range(NZ), key=lambda k: last[k]):
        run_until_received(lambda key: key[0] == DOWN and key[1] == dz)
        wait_across(DOWN, dz)
        zc = lax.rem(z + NZ - dz, NZ)
        rows = pl.ds(pl.multiple_of(zc * 256, 256), 256)
        fo[zc] = lax.dot_general(
            hid[...], w[DOWN, rows, :], (((1,), (1,)), ((), ())), preferred_element_type=F32
        ).astype(BF)
        for r in (2, 1, 3):
            ffn_copy(r, zc).start()
    run_until(1e9)
    for r in range(1, NT):
        pltpu.make_async_remote_copy(
            src_ref=rs2.at[r - 1], dst_ref=rs2.at[r - 1], send_sem=f_send.at[r],
            recv_sem=f_recv.at[r], device_id=partner, device_id_type=MESH,
        ).wait_recv()
    for n in range(NZ):
        cols = slice(n * 256, (n + 1) * 256)
        total = fo[n, mine, :].astype(F32)
        for r in range(NT - 1):
            total = total + rs2[r, n].astype(F32)
        out_ref[:, cols] = (mid[:, cols] + total).astype(BF)

    for a in (GATE, UP, DOWN):
        sent = w.at[a, pl.ds(0, SENT[a] * ROWS), :]
        pltpu.make_async_remote_copy(
            src_ref=sent, dst_ref=sent, send_sem=w_send.at[a], recv_sem=w_recv.at[a, 0, 0],
            device_id=partner, device_id_type=MESH,
        ).wait_send()
        for dz in range(NZ):
            whole = w.at[a, pl.ds(0, NX * ROWS), :]
            pltpu.make_async_remote_copy(
                src_ref=whole, dst_ref=whole, send_sem=d_send.at[a, dz],
                recv_sem=d_recv.at[a, dz], device_id=partner, device_id_type=MESH,
            ).wait_send()
    for r in range(1, NX * NC):
        group_copy(r).wait_send()
        back_copy(r).wait_send()
    for r in range(1, NZ):
        z_copy(r).wait_send()
    for r in range(1, NT):
        sum_copy(r).wait_send()
        norm_copy(r).wait_send()
        pltpu.make_async_remote_copy(
            src_ref=rs2.at[r - 1], dst_ref=rs2.at[r - 1], send_sem=f_send.at[r],
            recv_sem=f_recv.at[r], device_id=partner, device_id_type=MESH,
        ).wait_send()


DMA = pltpu.SemaphoreType.DMA


def body(
    queries, key_rows, value_rows, gate_input, log_decay, head_gain, out_weight, residual,
    mlp_gain, gate_weight, up_weight, down_weight,
):
    half = HD // 2
    offset = lax.axis_index(SP) * TOK
    positions = (offset + lax.iota(jnp.int32, TOK)).astype(F32)[:, None]
    freq = 10000.0 ** (-jnp.linspace(0.0, 1.0, half, dtype=F32))
    angles = positions * freq
    cosv, sinv = jnp.cos(angles), jnp.sin(angles)
    cosv = jnp.concatenate([cosv, cosv], axis=-1)
    sinv = jnp.concatenate([-sinv, sinv], axis=-1)
    res = lax.dynamic_slice_in_dim(residual, lax.axis_index("tp") * QT, QT, 0)
    vmem = pl.BlockSpec(memory_space=pltpu.VMEM)
    V = pltpu.VMEM
    return pl.pallas_call(
        kernel,
        out_shape=jax.ShapeDtypeStruct((QT, D), BF),
        in_specs=[vmem] * 14,
        out_specs=vmem,
        scratch_shapes=[
            V((3, D, FF), BF),
            V((TOK, HD), F32),
            V((TOK, HEADS * HD), BF),
            V((TOK, HEADS * HD), F32),
            V((TOK, HEADS * HD), BF),
            V((8, 80, HD), BF),
            V((8, 80, HD), BF),
            V((8, 64, HD), F32),
            V((80, HD), BF),
            V((8, 80, HD), BF),
            V((8, 64, HD), BF),
            V((8, 64, HD), BF),
            V((TOK, D), BF),
            V((NT - 1, QT, D), BF),
            V((TOK, D), BF),
            V((QT, D), F32),
            V((TOK, FF), F32),
            V((TOK, FF), F32),
            V((TOK, FF), BF),
            V((NZ, TOK, 256), BF),
            V((NT - 1, NZ, QT, 256), BF),
            DMA((3, NZ, NX)),
            DMA((3,)),
            DMA((3, NZ)),
            DMA((3, NZ)),
            DMA((8,)), DMA((8,)), DMA((8,)), DMA((8,)), DMA((8,)), DMA((8,)),
            DMA((NT,)), DMA((NT,)), DMA((NT,)), DMA((NT,)), DMA((NT,)), DMA((NT,)),
        ],
        compiler_params=pltpu.CompilerParams(
            collective_id=0, has_side_effects=True, vmem_limit_bytes=56 * 1024 * 1024
        ),
    )(
        queries, key_rows, value_rows, gate_input, log_decay, cosv, sinv, head_gain[None, :],
        out_weight, res, mlp_gain[None, :], gate_weight, up_weight, down_weight.T,
    )


def solution(mesh):
    finer = Mesh(mesh.devices.reshape(NZ, NX, NC, NT), ("z", "x", "c", "tp"))
    in_specs = (
        P(SP, "tp"), P(SP, "tp"), P(SP, "tp"), P(SP, "tp"), P(SP, "tp"), P("tp"), P("tp", None),
        P(SP, None), P(), P(SP, "tp"), P(SP, "tp"), P("tp", SP),
    )
    out_specs = P(("z", "x", "c", "tp"), None)
    return jax.shard_map(body, mesh=finer, in_specs=in_specs, out_specs=out_specs, check_vma=False)
```

```python
import heapq

import jax
import jax.numpy as jnp
import numpy as np
from jax import lax
from jax.experimental import pallas as pl
from jax.experimental.pallas import tpu as pltpu
from jax.sharding import Mesh
from jax.sharding import PartitionSpec as P

BF = jnp.bfloat16
F32 = jnp.float32
MESH = pl.DeviceIdType.MESH
HIGH = lax.Precision.HIGHEST
EPS = 1e-06

NZ, NX, NC, NT = 8, 4, 2, 4
SP = ("z", "x", "c")
TOK = 128
HD = 128
HEADS = 4
D = 2048
FF = 1408
ROWS = 32
QT = TOK // NT
GATE, UP, DOWN = 0, 1, 2

PIECE_US = 2.1
HOP_US = 4.0
LEAF_US = 2.0
LEAD = 1.0
LINKS = ("z+", "z-", "x+", "x-")
CODES = (
    16, 241, 134, 15, 144, 369, 6, 143, 272, 113, 138, 31, 32, 225, 150, 159, 160, 117, 10, 383,
    230, 47, 48, 253, 122, 175, 164, 97, 154, 27, 176, 209, 234, 379, 64, 213, 126, 63, 180, 101,
    54, 111, 40, 193, 238, 171, 188, 217, 70, 59, 76, 85, 186, 107, 288, 93, 198, 23, 204, 361,
    222, 39, 72, 245, 90, 251, 200, 81, 294, 303, 304, 345, 374, 359, 264, 353, 278, 268, 365, 299,
    310, 320, 329, 319, 350, 260, 285, 343, 282, 337, 312, 326, 335,
)


def sender_name(key, link):
    a, dz, dx = key
    if link == "z+":
        return (a, (dz - 1) % NZ, dx)
    if link == "z-":
        return (a, (dz + 1) % NZ, dx)
    if link == "x+":
        return (a, dz, (dx - 1) % NX)
    return (a, dz, (dx + 1) % NX)


def exchange_plan():
    onward = {}
    for turn, code in enumerate(CODES):
        key, link = (code // 128, code // 16 % 8, code // 4 % 4), LINKS[code % 4]
        onward.setdefault(sender_name(key, link), []).append((turn, link, key))
    pending = {link: [] for link in LINKS}
    free = dict.fromkeys(LINKS, 0.0)
    arrivals, ops, since = [], [], {}

    def ready(now, key):
        for turn, link, there in onward.get(key, ()):
            since[turn] = now
            heapq.heappush(pending[link], (turn, there))

    for a in (GATE, UP, DOWN):
        ready(0.0, (a, 0, 0))
    now = 0.0
    while True:
        for link, queue in pending.items():
            if queue and free[link] <= now:
                turn, key = heapq.heappop(queue)
                free[link] = now + PIECE_US
                ops.append((max(since[turn], now - LEAD * PIECE_US), 1, "send", link, key))
                heapq.heappush(arrivals, (now + PIECE_US + HOP_US, key))
        if not arrivals:
            break
        now = min([arrivals[0][0]] + [u for link, u in free.items() if pending[link] and u > now])
        while arrivals and arrivals[0][0] <= now + 1e-9:
            _, key = heapq.heappop(arrivals)
            ops.append((now, 0, "recv", None, key))
            ready(now, key)
    due = {}
    for time, _, kind, link, key in ops:
        if kind == "send":
            held = sender_name(key, link)
            due[held] = min(time, due.get(held, time))
    ops = [
        (due.get(key, time + LEAF_US), order, kind, link, key) if kind == "recv" else (time, order, kind, link, key)
        for time, order, kind, link, key in ops
    ]
    ops.sort(key=lambda op: (op[0], op[1]))
    return ops


PLAN = exchange_plan()
SENT = {a: sum(1 for op in PLAN if op[2] == "send" and op[4][0] == a) for a in (GATE, UP, DOWN)}

T_CONTRIB, T_GROUP, T_ALONG, T_BACK, T_SUM1, T_GATHER = 3.0, 8.0, 13.5, 18.0, 28.0, 36.0


def head_cols(h):
    return slice(h * HD, (h + 1) * HD)


def split_log(total):
    hi = total.astype(BF).astype(F32)
    rest = total - hi
    mid = rest.astype(BF).astype(F32)
    low = rest - mid
    i = lax.broadcasted_iota(jnp.int32, (16, HD), 0)
    return jnp.where(i == 0, hi, jnp.where(i == 1, mid, low)).astype(BF)


def join_log(tile):
    t = tile.astype(F32)
    return t[0:1] + t[1:2] + t[2:3]


def silu(v):
    return v * (1.0 / (1.0 + jnp.exp(-v)))


def kernel(
    q_hbm, k_hbm, v_hbm, gi_hbm, ld_hbm, freq_hbm, hg_hbm, ow_hbm, res_hbm, mg_hbm, gw_hbm, uw_hbm, dw_hbm,
    out_ref,
    q_ref, k_ref, v_ref, gi_ref, ld_ref, freq_ref, hg_ref, ow_ref, res_ref, mg_ref, gw_ref, uw_ref, dw_ref, in_sem,
    w, ldp, qrot, inner, ret, stout, stin, pre, zout, zin, bout, bin_, po, rs1, nfull, mid,
    gacc, uacc, hid, fo, rs2,
    w_recv, w_send, d_recv, d_send,
    g_recv, g_send, z_recv, z_send, b_recv, b_send, r_recv, r_send, n_recv, n_send, f_recv, f_send,
):
    z, x, c, t = lax.axis_index("z"), lax.axis_index("x"), lax.axis_index("c"), lax.axis_index("tp")
    pos = x * NC + c

    def group_peer(r):
        p = lax.rem(pos + r, NX * NC)
        return p, (z, lax.div(p, NC), lax.rem(p, NC), t)

    def z_peer(r):
        return (lax.rem(z + r, NZ), x, c, t)

    def tp_peer(r):
        j = lax.rem(t + r, NT)
        return j, (z, x, c, j)

    neighbours = {
        "z+": (lax.rem(z + 1, NZ), x, c, t),
        "z-": (lax.rem(z + NZ - 1, NZ), x, c, t),
        "x+": (z, lax.rem(x + 1, NX), c, t),
        "x-": (z, lax.rem(x + NX - 1, NX), c, t),
    }
    partner = (z, x, 1 - c, t)

    mine = pl.ds(pl.multiple_of(t * QT, QT), QT)
    inputs = {
        "gw": (gw_hbm, gw_ref), "uw": (uw_hbm, uw_ref), "dw": (dw_hbm, dw_ref), "freq": (freq_hbm, freq_ref),
        "ld": (ld_hbm, ld_ref), "k": (k_hbm, k_ref), "v": (v_hbm, v_ref), "q": (q_hbm, q_ref),
        "gi": (gi_hbm, gi_ref), "hg": (hg_hbm, hg_ref), "ow": (ow_hbm, ow_ref),
        "res": (res_hbm.at[mine, :], res_ref), "mg": (mg_hbm, mg_ref),
    }
    loads = {
        name: pltpu.make_async_copy(src, dst, in_sem.at[i]) for i, (name, (src, dst)) in enumerate(inputs.items())
    }
    for load in loads.values():
        load.start()

    def loaded(*names):
        for name in names:
            loads[name].wait()

    barrier = pltpu.get_barrier_semaphore()
    for r in range(1, NX * NC):
        pl.semaphore_signal(barrier, inc=1, device_id=group_peer(r)[1], device_id_type=MESH)
    for r in range(1, NZ):
        pl.semaphore_signal(barrier, inc=1, device_id=z_peer(r), device_id_type=MESH)
    for r in range(1, NT):
        pl.semaphore_signal(barrier, inc=1, device_id=tp_peer(r)[1], device_id_type=MESH)
    loaded("gw", "uw", "dw")
    pl.semaphore_wait(barrier, NX * NC - 1 + NZ - 1 + NT - 1)

    own = {GATE: gw_ref, UP: uw_ref, DOWN: dw_ref}

    def rows_of(dz, dx, core):
        sz = lax.rem(z + NZ - dz, NZ)
        sx = lax.rem(x + NX - dx, NX)
        return pl.ds(pl.multiple_of(((sz * NX + sx) * NC + core) * ROWS, ROWS), ROWS)

    def at_home(key):
        a, dz, dx = key
        return w.at[a, rows_of(dz, dx, c), :]

    def source(key):
        return own[key[0]] if key[1:] == (0, 0) else at_home(key)

    def hop(link, key):
        a, dz, dx = key
        held = sender_name(key, link)
        return pltpu.make_async_remote_copy(
            src_ref=source(held), dst_ref=at_home(held), send_sem=w_send.at[a],
            recv_sem=w_recv.at[a, dz, dx], device_id=neighbours[link], device_id_type=MESH,
        )

    def across(key):
        a, dz, dx = key
        return pltpu.make_async_remote_copy(
            src_ref=source(key), dst_ref=at_home(key), send_sem=d_send.at[a, dz],
            recv_sem=d_recv.at[a, dz], device_id=partner, device_id_type=MESH,
        )

    cursor = [0]

    def step(op):
        _, _, kind, link, key = op
        if kind == "send":
            hop(link, key).start()
        else:
            a, dz, dx = key
            pltpu.make_async_remote_copy(
                src_ref=at_home(key), dst_ref=at_home(key), send_sem=w_send.at[a],
                recv_sem=w_recv.at[a, dz, dx], device_id=partner, device_id_type=MESH,
            ).wait_recv()
            across(key).start()

    def run_until(time):
        while cursor[0] < len(PLAN) and PLAN[cursor[0]][0] <= time:
            step(PLAN[cursor[0]])
            cursor[0] += 1

    def run_until_received(wanted):
        last = max(i for i, op in enumerate(PLAN) if op[2] == "recv" and wanted(op[4]))
        while cursor[0] <= last:
            step(PLAN[cursor[0]])
            cursor[0] += 1

    def wait_across(a, dz):
        whole = w.at[a, pl.ds(0, NX * ROWS), :]
        pltpu.make_async_remote_copy(
            src_ref=whole, dst_ref=whole, send_sem=d_send.at[a, dz],
            recv_sem=d_recv.at[a, dz], device_id=partner, device_id_type=MESH,
        ).wait_recv()

    run_until(0.0)
    for a in (GATE, UP, DOWN):
        across((a, 0, 0)).start()

    loaded("freq")
    row = lax.broadcasted_iota(jnp.int32, (TOK, HD), 0) + ((z * NX + x) * NC + c) * TOK
    angles = row.astype(F32) * freq_ref[...]
    cosv = jnp.cos(angles)
    sinv = jnp.sin(angles)
    sinv = jnp.where(lax.broadcasted_iota(jnp.int32, (TOK, HD), 1) < HD // 2, -sinv, sinv)
    loaded("ld", "k", "v")
    ldp[...] = jnp.zeros((TOK, HD), F32)
    ldp[0:HEADS, :] = ld_ref[...]
    ti = lax.broadcasted_iota(jnp.int32, (TOK, TOK), 0)
    si = lax.broadcasted_iota(jnp.int32, (TOK, TOK), 1)
    lower = si <= ti
    cum_t = jnp.dot(ldp[...], (ti <= si).astype(F32), precision=HIGH, preferred_element_type=F32)
    cum = cum_t.T
    krots = []
    for h in range(HEADS):
        kf = k_ref[:, head_cols(h)].astype(F32)
        krot = ((kf * cosv + pltpu.roll(kf, HD // 2, 1) * sinv) * HD ** (-0.5)).astype(BF)
        krots.append(krot)
        col = cum[:, h : h + 1]
        last = cum[TOK - 1 : TOK, h : h + 1]
        kw = (krot.astype(F32) * jnp.exp(last - col)).astype(BF)
        contrib = jnp.dot(kw.T, v_ref[:, head_cols(h)], preferred_element_type=F32)
        logs = split_log(jnp.broadcast_to(last, (1, HD)))
        for half in range(2):
            stout[2 * h + half, 0:64, :] = contrib[64 * half : 64 * half + 64].astype(BF)
            stout[2 * h + half, 64:80, :] = logs
    for a in (GATE, UP, DOWN):
        w[a, rows_of(0, 0, c), :] = own[a][...]
    run_until(T_CONTRIB)

    def group_copy(r):
        p, peer = group_peer(r)
        return pltpu.make_async_remote_copy(
            src_ref=stout.at[p], dst_ref=stin.at[pos], send_sem=g_send.at[r],
            recv_sem=g_recv.at[r], device_id=peer, device_id_type=MESH,
        )

    for r in range(1, NX * NC):
        group_copy(r).start()
    stin[pos] = stout[pos]

    loaded("q")
    for h in range(HEADS):
        qf = q_ref[:, head_cols(h)].astype(F32)
        qr = (qf * cosv + pltpu.roll(qf, HD // 2, 1) * sinv).astype(BF)
        qrot[:, head_cols(h)] = qr
        spread = cum[:, h : h + 1] - cum_t[h : h + 1, :]
        weight = jnp.where(lower, jnp.exp(jnp.where(lower, spread, 0.0)), 0.0)
        scores = lax.dot_general(qr, krots[h], (((1,), (1,)), ((), ())), preferred_element_type=F32)
        probs = (scores * weight).astype(BF)
        inner[:, head_cols(h)] = jnp.dot(probs, v_ref[:, head_cols(h)], preferred_element_type=F32)
    run_until(T_GROUP)

    for r in range(1, NX * NC):
        group_copy(r).wait_recv()
    run = jnp.zeros((64, HD), F32)
    sofar = jnp.zeros((1, HD), F32)
    reach = []
    for p in range(NX * NC):
        pre[p] = run
        reach.append(sofar)
        log = join_log(stin[p, 64:80, :])
        run = run * jnp.exp(log) + stin[p, 0:64, :].astype(F32)
        sofar = sofar + log
    zout[0:64, :] = run.astype(BF)
    zout[64:80, :] = split_log(sofar)

    def z_copy(r):
        return pltpu.make_async_remote_copy(
            src_ref=zout, dst_ref=zin.at[z], send_sem=z_send.at[r],
            recv_sem=z_recv.at[r], device_id=z_peer(r), device_id_type=MESH,
        )

    for r in range(1, NZ):
        z_copy(r).start()
    zin[z] = zout[...]
    run_until(T_ALONG)
    for r in range(1, NZ):
        z_copy(r).wait_recv()
    came = jnp.zeros((64, HD), F32)
    for s in range(NZ):
        log = join_log(zin[s, 64:80, :])
        came = jnp.where(s < z, came * jnp.exp(log) + zin[s, 0:64, :].astype(F32), came)
    for p in range(NX * NC):
        bout[p] = (pre[p] + jnp.exp(reach[p]) * came).astype(BF)

    def back_copy(r):
        p, peer = group_peer(r)
        return pltpu.make_async_remote_copy(
            src_ref=bout.at[p], dst_ref=bin_.at[pos], send_sem=b_send.at[r],
            recv_sem=b_recv.at[r], device_id=peer, device_id_type=MESH,
        )

    for r in range(1, NX * NC):
        back_copy(r).start()
    bin_[pos] = bout[pos]
    run_until(T_BACK)
    for r in range(1, NX * NC):
        back_copy(r).wait_recv()

    loaded("gi", "hg", "ow", "res", "mg")
    for h in range(HEADS):
        before = bin_[2 * h : 2 * h + 2].reshape(HD, HD)
        cross = jnp.dot(qrot[:, head_cols(h)], before, preferred_element_type=F32)
        res = inner[:, head_cols(h)] + cross * jnp.exp(cum[:, h : h + 1])
        scale = lax.rsqrt(jnp.mean(res * res, axis=-1, keepdims=True) + EPS)
        gain = hg_ref[:, head_cols(h)]
        ret[:, head_cols(h)] = (
            res * scale * gain * silu(gi_ref[:, head_cols(h)].astype(F32))
        ).astype(BF)
    for n in range(0, D, 512):
        po[:, n : n + 512] = jnp.dot(
            ret[...], ow_ref[:, n : n + 512], preferred_element_type=F32
        ).astype(BF)

    def sum_copy(r):
        j, peer = tp_peer(r)
        return pltpu.make_async_remote_copy(
            src_ref=po.at[pl.ds(pl.multiple_of(j * QT, QT), QT), :], dst_ref=rs1.at[r - 1],
            send_sem=r_send.at[r], recv_sem=r_recv.at[r], device_id=peer, device_id_type=MESH,
        )

    for r in (2, 1, 3):
        sum_copy(r).start()
    run_until(T_SUM1)
    for r in range(1, NT):
        sum_copy(r).wait_recv()
    mixed = po[mine, :].astype(F32)
    for r in range(NT - 1):
        mixed = mixed + rs1[r].astype(F32)
    middle = (res_ref[...].astype(F32) + mixed).astype(BF).astype(F32)
    mid[...] = middle
    scale = lax.rsqrt(jnp.mean(middle * middle, axis=-1, keepdims=True) + EPS)
    nfull[mine, :] = (middle * scale * mg_ref[...]).astype(BF)

    def norm_copy(r):
        return pltpu.make_async_remote_copy(
            src_ref=nfull.at[mine, :], dst_ref=nfull.at[mine, :],
            send_sem=n_send.at[r], recv_sem=n_recv.at[r], device_id=tp_peer(r)[1],
            device_id_type=MESH,
        )

    def norm_arrived(r):
        rows = nfull.at[pl.ds(pl.multiple_of(lax.rem(t + NT - r, NT) * QT, QT), QT), :]
        pltpu.make_async_remote_copy(
            src_ref=rows, dst_ref=rows, send_sem=n_send.at[r], recv_sem=n_recv.at[r],
            device_id=partner, device_id_type=MESH,
        ).wait_recv()

    for r in (2, 1, 3):
        norm_copy(r).start()
    run_until(T_GATHER)
    for r in range(1, NT):
        norm_arrived(r)

    run_until_received(lambda key: key[0] != DOWN)
    for a in (GATE, UP):
        for dz in range(NZ):
            wait_across(a, dz)
    clock = PLAN[cursor[0] - 1][0]
    for n in range(NZ):
        rows = slice(n * 256, (n + 1) * 256)
        for a, acc in ((GATE, gacc), (UP, uacc)):
            term = jnp.dot(nfull[:, rows], w[a, rows, :], preferred_element_type=F32)
            acc[...] = term if n == 0 else acc[...] + term
        clock += 0.6
        run_until(clock)
    hid[...] = (silu(gacc[...]) * uacc[...]).astype(BF)

    def ffn_copy(r, zc):
        j, peer = tp_peer(r)
        return pltpu.make_async_remote_copy(
            src_ref=fo.at[zc, pl.ds(pl.multiple_of(j * QT, QT), QT), :], dst_ref=rs2.at[r - 1, zc],
            send_sem=f_send.at[r], recv_sem=f_recv.at[r], device_id=peer, device_id_type=MESH,
        )

    last = {}
    for i, op in enumerate(PLAN):
        if op[2] == "recv" and op[4][0] == DOWN:
            last[op[4][1]] = i
    for dz in sorted(range(NZ), key=lambda k: last[k]):
        run_until_received(lambda key: key[0] == DOWN and key[1] == dz)
        wait_across(DOWN, dz)
        zc = lax.rem(z + NZ - dz, NZ)
        rows = pl.ds(pl.multiple_of(zc * 256, 256), 256)
        fo[zc] = lax.dot_general(
            hid[...], w[DOWN, rows, :], (((1,), (1,)), ((), ())), preferred_element_type=F32
        ).astype(BF)
        for r in (2, 1, 3):
            ffn_copy(r, zc).start()
    run_until(1e9)
    for r in range(1, NT):
        pltpu.make_async_remote_copy(
            src_ref=rs2.at[r - 1], dst_ref=rs2.at[r - 1], send_sem=f_send.at[r],
            recv_sem=f_recv.at[r], device_id=partner, device_id_type=MESH,
        ).wait_recv()
    for n in range(NZ):
        cols = slice(n * 256, (n + 1) * 256)
        total = fo[n, mine, :].astype(F32)
        for r in range(NT - 1):
            total = total + rs2[r, n].astype(F32)
        out_ref[:, cols] = (mid[:, cols] + total).astype(BF)

    for a in (GATE, UP, DOWN):
        sent = w.at[a, pl.ds(0, SENT[a] * ROWS), :]
        pltpu.make_async_remote_copy(
            src_ref=sent, dst_ref=sent, send_sem=w_send.at[a], recv_sem=w_recv.at[a, 0, 0],
            device_id=partner, device_id_type=MESH,
        ).wait_send()
        for dz in range(NZ):
            whole = w.at[a, pl.ds(0, NX * ROWS), :]
            pltpu.make_async_remote_copy(
                src_ref=whole, dst_ref=whole, send_sem=d_send.at[a, dz],
                recv_sem=d_recv.at[a, dz], device_id=partner, device_id_type=MESH,
            ).wait_send()
    for r in range(1, NX * NC):
        group_copy(r).wait_send()
        back_copy(r).wait_send()
    for r in range(1, NZ):
        z_copy(r).wait_send()
    for r in range(1, NT):
        sum_copy(r).wait_send()
        norm_copy(r).wait_send()
        pltpu.make_async_remote_copy(
            src_ref=rs2.at[r - 1], dst_ref=rs2.at[r - 1], send_sem=f_send.at[r],
            recv_sem=f_recv.at[r], device_id=partner, device_id_type=MESH,
        ).wait_send()


DMA = pltpu.SemaphoreType.DMA


def body(
    queries, key_rows, value_rows, gate_input, log_decay, head_gain, out_weight, residual,
    mlp_gain, gate_weight, up_weight, down_weight,
):
    freq = np.float32(10000.0 ** -np.linspace(0.0, 1.0, HD // 2))
    freq = jnp.asarray(np.concatenate([freq, freq])[None, :])
    vmem = pl.BlockSpec(memory_space=pltpu.VMEM)
    V = pltpu.VMEM
    return pl.pallas_call(
        kernel,
        out_shape=jax.ShapeDtypeStruct((QT, D), BF),
        in_specs=[pl.BlockSpec(memory_space=pl.ANY)] * 13,
        out_specs=vmem,
        scratch_shapes=[
            V((TOK, HEADS * HD), BF), V((TOK, HEADS * HD), BF), V((TOK, HEADS * HD), BF), V((TOK, HEADS * HD), BF),
            V((HEADS, TOK), F32), V((1, HD), F32), V((1, HEADS * HD), F32), V((HEADS * HD, D), BF), V((QT, D), BF),
            V((1, D), F32), V((ROWS, FF), BF), V((ROWS, FF), BF), V((ROWS, FF), BF), DMA((13,)),
            V((3, D, FF), BF),
            V((TOK, HD), F32),
            V((TOK, HEADS * HD), BF),
            V((TOK, HEADS * HD), F32),
            V((TOK, HEADS * HD), BF),
            V((8, 80, HD), BF),
            V((8, 80, HD), BF),
            V((8, 64, HD), F32),
            V((80, HD), BF),
            V((8, 80, HD), BF),
            V((8, 64, HD), BF),
            V((8, 64, HD), BF),
            V((TOK, D), BF),
            V((NT - 1, QT, D), BF),
            V((TOK, D), BF),
            V((QT, D), F32),
            V((TOK, FF), F32),
            V((TOK, FF), F32),
            V((TOK, FF), BF),
            V((NZ, TOK, 256), BF),
            V((NT - 1, NZ, QT, 256), BF),
            DMA((3, NZ, NX)),
            DMA((3,)),
            DMA((3, NZ)),
            DMA((3, NZ)),
            DMA((8,)), DMA((8,)), DMA((8,)), DMA((8,)), DMA((8,)), DMA((8,)),
            DMA((NT,)), DMA((NT,)), DMA((NT,)), DMA((NT,)), DMA((NT,)), DMA((NT,)),
        ],
        compiler_params=pltpu.CompilerParams(
            collective_id=0, has_side_effects=True, vmem_limit_bytes=56 * 1024 * 1024
        ),
    )(
        queries, key_rows, value_rows, gate_input, log_decay.T, freq, head_gain[None, :], out_weight, residual,
        mlp_gain[None, :], gate_weight, up_weight, down_weight.T,
    )


def solution(mesh):
    finer = Mesh(mesh.devices.reshape(NZ, NX, NC, NT), ("z", "x", "c", "tp"))
    in_specs = (
        P(SP, "tp"), P(SP, "tp"), P(SP, "tp"), P(SP, "tp"), P(SP, "tp"), P("tp"), P("tp", None),
        P(SP, None), P(), P(SP, "tp"), P(SP, "tp"), P("tp", SP),
    )
    out_specs = P(("z", "x", "c", "tp"), None)
    return jax.shard_map(body, mesh=finer, in_specs=in_specs, out_specs=out_specs, check_vma=False)
```

```python
import heapq

import jax
import jax.numpy as jnp
import numpy as np
from jax import lax
from jax.experimental import pallas as pl
from jax.experimental.pallas import tpu as pltpu
from jax.sharding import Mesh
from jax.sharding import PartitionSpec as P

BF = jnp.bfloat16
F32 = jnp.float32
MESH = pl.DeviceIdType.MESH
HIGH = lax.Precision.HIGHEST
EPS = 1e-06

NZ, NX, NC, NT = 8, 4, 2, 4
SP = ("z", "x", "c")
TOK = 128
HD = 128
HEADS = 4
D = 2048
FF = 1408
ROWS = 32
QT = TOK // NT
GATE, UP, DOWN = 0, 1, 2

PIECE_US = 2.1
HOP_US = 4.0
LEAF_US = 0.5
LEAD = 1.0
LINKS = ("z+", "z-", "x+", "x-")
CODES = (
    16, 241, 6, 143, 272, 113, 134, 271, 144, 369, 10, 31, 32, 225, 118, 127, 156, 97, 374, 255,
    160, 245, 14, 239, 48, 209, 38, 111, 172, 81, 378, 27, 284, 101, 166, 47, 20, 93, 214, 63,
    148, 65, 122, 171, 176, 193, 106, 235, 300, 77, 218, 59, 228, 197, 70, 251, 40, 85, 154, 191,
    316, 89, 290, 283, 72, 357, 202, 383, 180, 53, 222, 187, 204, 137, 306, 279, 332, 341, 362, 355,
    296, 365, 294, 315, 260, 265, 310, 331, 320, 325, 346, 339, 349,
)


def sender_name(key, link):
    a, dz, dx = key
    if link == "z+":
        return (a, (dz - 1) % NZ, dx)
    if link == "z-":
        return (a, (dz + 1) % NZ, dx)
    if link == "x+":
        return (a, dz, (dx - 1) % NX)
    return (a, dz, (dx + 1) % NX)


def exchange_plan():
    onward = {}
    for turn, code in enumerate(CODES):
        key, link = (code // 128, code // 16 % 8, code // 4 % 4), LINKS[code % 4]
        onward.setdefault(sender_name(key, link), []).append((turn, link, key))
    pending = {link: [] for link in LINKS}
    free = dict.fromkeys(LINKS, 0.0)
    arrivals, ops, since = [], [], {}

    def ready(now, key):
        for turn, link, there in onward.get(key, ()):
            since[turn] = now
            heapq.heappush(pending[link], (turn, there))

    for a in (GATE, UP, DOWN):
        ready(0.0, (a, 0, 0))
    now = 0.0
    while True:
        for link, queue in pending.items():
            if queue and free[link] <= now:
                turn, key = heapq.heappop(queue)
                free[link] = now + PIECE_US
                ops.append((max(since[turn], now - LEAD * PIECE_US), 1, "send", link, key))
                heapq.heappush(arrivals, (now + PIECE_US + HOP_US, key))
        if not arrivals:
            break
        now = min([arrivals[0][0]] + [u for link, u in free.items() if pending[link] and u > now])
        while arrivals and arrivals[0][0] <= now + 1e-9:
            _, key = heapq.heappop(arrivals)
            ops.append((now, 0, "recv", None, key))
            ready(now, key)
    due = {}
    for time, _, kind, link, key in ops:
        if kind == "send":
            held = sender_name(key, link)
            due[held] = min(time, due.get(held, time))
    ops = [
        (due.get(key, time + LEAF_US), order, kind, link, key) if kind == "recv" else (time, order, kind, link, key)
        for time, order, kind, link, key in ops
    ]
    ops.sort(key=lambda op: (op[0], op[1]))
    return ops


PLAN = exchange_plan()
SENT = {a: sum(1 for op in PLAN if op[2] == "send" and op[4][0] == a) for a in (GATE, UP, DOWN)}

T_CONTRIB, T_GROUP, T_ALONG, T_BACK, T_SUM1, T_GATHER = 3.0, 10.0, 16.5, 22.5, 32.5, 41.0


def head_cols(h):
    return slice(h * HD, (h + 1) * HD)


def split_log(total):
    hi = total.astype(BF).astype(F32)
    rest = total - hi
    mid = rest.astype(BF).astype(F32)
    low = rest - mid
    i = lax.broadcasted_iota(jnp.int32, (16, HD), 0)
    return jnp.where(i == 0, hi, jnp.where(i == 1, mid, low)).astype(BF)


def join_log(tile):
    t = tile.astype(F32)
    return t[0:1] + t[1:2] + t[2:3]


def silu(v):
    return v * (1.0 / (1.0 + jnp.exp(-v)))


def kernel(
    q_hbm, k_hbm, v_hbm, gi_hbm, ld_hbm, freq_hbm, hg_hbm, ow_hbm, res_hbm, mg_hbm, gw_hbm, uw_hbm, dw_hbm,
    out_ref,
    q_ref, k_ref, v_ref, gi_ref, ld_ref, freq_ref, hg_ref, ow_ref, res_ref, mg_ref, gw_ref, uw_ref, dw_ref, in_sem,
    w, ldp, qrot, inner, ret, stout, stin, pre, came_ref, zout, zin, bout, bin_, po, rs1, nfull, mid,
    gacc, uacc, hid, fo, rs2,
    w_recv, w_send, d_recv, d_send,
    g_recv, g_send, z_recv, z_send, b_recv, b_send, r_recv, r_send, n_recv, n_send, f_recv, f_send,
):
    z, x, c, t = lax.axis_index("z"), lax.axis_index("x"), lax.axis_index("c"), lax.axis_index("tp")
    pos = x * NC + c

    def group_peer(r):
        p = lax.rem(pos + r, NX * NC)
        return p, (z, lax.div(p, NC), lax.rem(p, NC), t)

    def z_peer(r):
        return (lax.rem(z + r, NZ), x, c, t)

    def tp_peer(r):
        j = lax.rem(t + r, NT)
        return j, (z, x, c, j)

    neighbours = {
        "z+": (lax.rem(z + 1, NZ), x, c, t),
        "z-": (lax.rem(z + NZ - 1, NZ), x, c, t),
        "x+": (z, lax.rem(x + 1, NX), c, t),
        "x-": (z, lax.rem(x + NX - 1, NX), c, t),
    }
    partner = (z, x, 1 - c, t)

    mine = pl.ds(pl.multiple_of(t * QT, QT), QT)
    inputs = {
        "gw": (gw_hbm, gw_ref), "uw": (uw_hbm, uw_ref), "dw": (dw_hbm, dw_ref), "freq": (freq_hbm, freq_ref),
        "ld": (ld_hbm, ld_ref), "k": (k_hbm, k_ref), "v": (v_hbm, v_ref), "q": (q_hbm, q_ref),
        "gi": (gi_hbm, gi_ref), "hg": (hg_hbm, hg_ref), "ow": (ow_hbm, ow_ref),
        "res": (res_hbm.at[mine, :], res_ref), "mg": (mg_hbm, mg_ref),
    }
    loads = {
        name: pltpu.make_async_copy(src, dst, in_sem.at[i]) for i, (name, (src, dst)) in enumerate(inputs.items())
    }
    for load in loads.values():
        load.start()

    def loaded(*names):
        for name in names:
            loads[name].wait()

    barrier = pltpu.get_barrier_semaphore()
    for r in range(1, NX * NC):
        pl.semaphore_signal(barrier, inc=1, device_id=group_peer(r)[1], device_id_type=MESH)
    for r in range(1, NZ):
        pl.semaphore_signal(barrier, inc=1, device_id=z_peer(r), device_id_type=MESH)
    for r in range(1, NT):
        pl.semaphore_signal(barrier, inc=1, device_id=tp_peer(r)[1], device_id_type=MESH)
    loaded("gw", "uw", "dw")
    pl.semaphore_wait(barrier, NX * NC - 1 + NZ - 1 + NT - 1)

    own = {GATE: gw_ref, UP: uw_ref, DOWN: dw_ref}

    def rows_of(dz, dx, core):
        sz = lax.rem(z + NZ - dz, NZ)
        sx = lax.rem(x + NX - dx, NX)
        return pl.ds(pl.multiple_of(((sz * NX + sx) * NC + core) * ROWS, ROWS), ROWS)

    def at_home(key):
        a, dz, dx = key
        return w.at[a, rows_of(dz, dx, c), :]

    def source(key):
        return own[key[0]] if key[1:] == (0, 0) else at_home(key)

    def hop(link, key):
        a, dz, dx = key
        held = sender_name(key, link)
        return pltpu.make_async_remote_copy(
            src_ref=source(held), dst_ref=at_home(held), send_sem=w_send.at[a],
            recv_sem=w_recv.at[a, dz, dx], device_id=neighbours[link], device_id_type=MESH,
        )

    def across(key):
        a, dz, dx = key
        return pltpu.make_async_remote_copy(
            src_ref=source(key), dst_ref=at_home(key), send_sem=d_send.at[a, dz],
            recv_sem=d_recv.at[a, dz], device_id=partner, device_id_type=MESH,
        )

    cursor = [0]

    def step(op):
        _, _, kind, link, key = op
        if kind == "send":
            hop(link, key).start()
        else:
            a, dz, dx = key
            pltpu.make_async_remote_copy(
                src_ref=at_home(key), dst_ref=at_home(key), send_sem=w_send.at[a],
                recv_sem=w_recv.at[a, dz, dx], device_id=partner, device_id_type=MESH,
            ).wait_recv()
            across(key).start()

    def run_until(time):
        while cursor[0] < len(PLAN) and PLAN[cursor[0]][0] <= time:
            step(PLAN[cursor[0]])
            cursor[0] += 1

    def run_until_received(wanted):
        last = max(i for i, op in enumerate(PLAN) if op[2] == "recv" and wanted(op[4]))
        while cursor[0] <= last:
            step(PLAN[cursor[0]])
            cursor[0] += 1

    def wait_across(a, dz):
        whole = w.at[a, pl.ds(0, NX * ROWS), :]
        pltpu.make_async_remote_copy(
            src_ref=whole, dst_ref=whole, send_sem=d_send.at[a, dz],
            recv_sem=d_recv.at[a, dz], device_id=partner, device_id_type=MESH,
        ).wait_recv()

    run_until(0.0)
    for a in (GATE, UP, DOWN):
        across((a, 0, 0)).start()

    loaded("freq")
    row = lax.broadcasted_iota(jnp.int32, (TOK, HD), 0) + ((z * NX + x) * NC + c) * TOK
    angles = row.astype(F32) * freq_ref[...]
    cosv = jnp.cos(angles)
    sinv = jnp.sin(angles)
    sinv = jnp.where(lax.broadcasted_iota(jnp.int32, (TOK, HD), 1) < HD // 2, -sinv, sinv)
    loaded("ld", "k", "v")
    ldp[...] = jnp.zeros((TOK, HD), F32)
    ldp[0:HEADS, :] = ld_ref[...]
    ti = lax.broadcasted_iota(jnp.int32, (TOK, TOK), 0)
    si = lax.broadcasted_iota(jnp.int32, (TOK, TOK), 1)
    lower = si <= ti
    cum_t = jnp.dot(ldp[...], (ti <= si).astype(F32), precision=HIGH, preferred_element_type=F32)
    cum = cum_t.T
    krots = []
    for h in range(HEADS):
        kf = k_ref[:, head_cols(h)].astype(F32)
        krot = ((kf * cosv + pltpu.roll(kf, HD // 2, 1) * sinv) * HD ** (-0.5)).astype(BF)
        krots.append(krot)
        col = cum[:, h : h + 1]
        last = cum[TOK - 1 : TOK, h : h + 1]
        kw = (krot.astype(F32) * jnp.exp(last - col)).astype(BF)
        contrib = jnp.dot(kw.T, v_ref[:, head_cols(h)], preferred_element_type=F32)
        logs = split_log(jnp.broadcast_to(last, (1, HD)))
        for half in range(2):
            stout[2 * h + half, 0:64, :] = contrib[64 * half : 64 * half + 64].astype(BF)
            stout[2 * h + half, 64:80, :] = logs
    for a in (GATE, UP, DOWN):
        w[a, rows_of(0, 0, c), :] = own[a][...]
    run_until(T_CONTRIB)

    def group_copy(r):
        p, peer = group_peer(r)
        return pltpu.make_async_remote_copy(
            src_ref=stout.at[p], dst_ref=stin.at[pos], send_sem=g_send.at[r],
            recv_sem=g_recv.at[r], device_id=peer, device_id_type=MESH,
        )

    for r in range(1, NX * NC):
        group_copy(r).start()
    stin[pos] = stout[pos]

    loaded("q")
    for h in range(HEADS):
        qf = q_ref[:, head_cols(h)].astype(F32)
        qr = (qf * cosv + pltpu.roll(qf, HD // 2, 1) * sinv).astype(BF)
        qrot[:, head_cols(h)] = qr
        spread = cum[:, h : h + 1] - cum_t[h : h + 1, :]
        weight = jnp.where(lower, jnp.exp(jnp.where(lower, spread, 0.0)), 0.0)
        scores = lax.dot_general(qr, krots[h], (((1,), (1,)), ((), ())), preferred_element_type=F32)
        probs = (scores * weight).astype(BF)
        inner[:, head_cols(h)] = jnp.dot(probs, v_ref[:, head_cols(h)], preferred_element_type=F32)
    run_until(T_GROUP)

    for r in range(1, NX * NC):
        group_copy(r).wait_recv()
    run = jnp.zeros((64, HD), F32)
    sofar = jnp.zeros((1, HD), F32)
    reach = []
    for p in range(NX * NC):
        pre[p] = run
        reach.append(sofar)
        log = join_log(stin[p, 64:80, :])
        run = run * jnp.exp(log) + stin[p, 0:64, :].astype(F32)
        sofar = sofar + log
    zout[0:64, :] = run.astype(BF)
    zout[64:80, :] = split_log(sofar)

    def z_copy(r):
        return pltpu.make_async_remote_copy(
            src_ref=zout, dst_ref=zin.at[z], send_sem=z_send.at[r],
            recv_sem=z_recv.at[r], device_id=z_peer(r), device_id_type=MESH,
        )

    for r in range(1, NZ):
        @pl.when(z + r < NZ)
        def _():
            z_copy(r).start()
    run_until(T_ALONG)
    for r in range(1, NZ):
        @pl.when(z >= r)
        def _():
            z_copy(r).wait_recv()
    came_ref[...] = jnp.zeros((64, HD), F32)
    for s in range(NZ - 1):
        @pl.when(s < z)
        def _():
            decay = jnp.exp(join_log(zin[s, 64:80, :]))
            came_ref[...] = came_ref[...] * decay + zin[s, 0:64, :].astype(F32)
    came = came_ref[...]
    for p in range(NX * NC):
        bout[p] = (pre[p] + jnp.exp(reach[p]) * came).astype(BF)

    def back_copy(r):
        p, peer = group_peer(r)
        return pltpu.make_async_remote_copy(
            src_ref=bout.at[p], dst_ref=bin_.at[pos], send_sem=b_send.at[r],
            recv_sem=b_recv.at[r], device_id=peer, device_id_type=MESH,
        )

    for r in range(1, NX * NC):
        back_copy(r).start()
    bin_[pos] = bout[pos]
    run_until(T_BACK)
    for r in range(1, NX * NC):
        back_copy(r).wait_recv()

    loaded("gi", "hg", "ow", "res", "mg")
    for h in range(HEADS):
        before = bin_[2 * h : 2 * h + 2].reshape(HD, HD)
        cross = jnp.dot(qrot[:, head_cols(h)], before, preferred_element_type=F32)
        res = inner[:, head_cols(h)] + cross * jnp.exp(cum[:, h : h + 1])
        scale = lax.rsqrt(jnp.mean(res * res, axis=-1, keepdims=True) + EPS)
        gain = hg_ref[:, head_cols(h)]
        ret[:, head_cols(h)] = (
            res * scale * gain * silu(gi_ref[:, head_cols(h)].astype(F32))
        ).astype(BF)
    for n in range(0, D, 512):
        po[:, n : n + 512] = jnp.dot(
            ret[...], ow_ref[:, n : n + 512], preferred_element_type=F32
        ).astype(BF)

    def sum_copy(r):
        j, peer = tp_peer(r)
        return pltpu.make_async_remote_copy(
            src_ref=po.at[pl.ds(pl.multiple_of(j * QT, QT), QT), :], dst_ref=rs1.at[r - 1],
            send_sem=r_send.at[r], recv_sem=r_recv.at[r], device_id=peer, device_id_type=MESH,
        )

    for r in (2, 1, 3):
        sum_copy(r).start()
    run_until(T_SUM1)
    for r in range(1, NT):
        sum_copy(r).wait_recv()
    mixed = po[mine, :].astype(F32)
    for r in range(NT - 1):
        mixed = mixed + rs1[r].astype(F32)
    middle = (res_ref[...].astype(F32) + mixed).astype(BF).astype(F32)
    mid[...] = middle
    scale = lax.rsqrt(jnp.mean(middle * middle, axis=-1, keepdims=True) + EPS)
    nfull[mine, :] = (middle * scale * mg_ref[...]).astype(BF)

    def norm_copy(r):
        return pltpu.make_async_remote_copy(
            src_ref=nfull.at[mine, :], dst_ref=nfull.at[mine, :],
            send_sem=n_send.at[r], recv_sem=n_recv.at[r], device_id=tp_peer(r)[1],
            device_id_type=MESH,
        )

    def norm_arrived(r):
        rows = nfull.at[pl.ds(pl.multiple_of(lax.rem(t + NT - r, NT) * QT, QT), QT), :]
        pltpu.make_async_remote_copy(
            src_ref=rows, dst_ref=rows, send_sem=n_send.at[r], recv_sem=n_recv.at[r],
            device_id=partner, device_id_type=MESH,
        ).wait_recv()

    for r in (2, 1, 3):
        norm_copy(r).start()
    run_until(T_GATHER)
    for r in range(1, NT):
        norm_arrived(r)

    run_until_received(lambda key: key[0] != DOWN)
    for a in (GATE, UP):
        for dz in range(NZ):
            wait_across(a, dz)
    clock = PLAN[cursor[0] - 1][0]
    for n in range(NZ):
        rows = slice(n * 256, (n + 1) * 256)
        for a, acc in ((GATE, gacc), (UP, uacc)):
            term = jnp.dot(nfull[:, rows], w[a, rows, :], preferred_element_type=F32)
            acc[...] = term if n == 0 else acc[...] + term
        clock += 0.6
        run_until(clock)
    hid[...] = (silu(gacc[...]) * uacc[...]).astype(BF)

    def ffn_copy(r, zc):
        j, peer = tp_peer(r)
        return pltpu.make_async_remote_copy(
            src_ref=fo.at[zc, pl.ds(pl.multiple_of(j * QT, QT), QT), :], dst_ref=rs2.at[r - 1, zc],
            send_sem=f_send.at[r], recv_sem=f_recv.at[r], device_id=peer, device_id_type=MESH,
        )

    last = {}
    for i, op in enumerate(PLAN):
        if op[2] == "recv" and op[4][0] == DOWN:
            last[op[4][1]] = i
    for dz in sorted(range(NZ), key=lambda k: last[k]):
        run_until_received(lambda key: key[0] == DOWN and key[1] == dz)
        wait_across(DOWN, dz)
        zc = lax.rem(z + NZ - dz, NZ)
        rows = pl.ds(pl.multiple_of(zc * 256, 256), 256)
        fo[zc] = lax.dot_general(
            hid[...], w[DOWN, rows, :], (((1,), (1,)), ((), ())), preferred_element_type=F32
        ).astype(BF)
        for r in (2, 1, 3):
            ffn_copy(r, zc).start()
    run_until(1e9)
    for r in range(1, NT):
        pltpu.make_async_remote_copy(
            src_ref=rs2.at[r - 1], dst_ref=rs2.at[r - 1], send_sem=f_send.at[r],
            recv_sem=f_recv.at[r], device_id=partner, device_id_type=MESH,
        ).wait_recv()
    for n in range(NZ):
        cols = slice(n * 256, (n + 1) * 256)
        total = fo[n, mine, :].astype(F32)
        for r in range(NT - 1):
            total = total + rs2[r, n].astype(F32)
        out_ref[:, cols] = (mid[:, cols] + total).astype(BF)

    for a in (GATE, UP, DOWN):
        sent = w.at[a, pl.ds(0, SENT[a] * ROWS), :]
        pltpu.make_async_remote_copy(
            src_ref=sent, dst_ref=sent, send_sem=w_send.at[a], recv_sem=w_recv.at[a, 0, 0],
            device_id=partner, device_id_type=MESH,
        ).wait_send()
        for dz in range(NZ):
            whole = w.at[a, pl.ds(0, NX * ROWS), :]
            pltpu.make_async_remote_copy(
                src_ref=whole, dst_ref=whole, send_sem=d_send.at[a, dz],
                recv_sem=d_recv.at[a, dz], device_id=partner, device_id_type=MESH,
            ).wait_send()
    for r in range(1, NX * NC):
        group_copy(r).wait_send()
        back_copy(r).wait_send()
    for r in range(1, NZ):
        @pl.when(z + r < NZ)
        def _():
            z_copy(r).wait_send()
    for r in range(1, NT):
        sum_copy(r).wait_send()
        norm_copy(r).wait_send()
        pltpu.make_async_remote_copy(
            src_ref=rs2.at[r - 1], dst_ref=rs2.at[r - 1], send_sem=f_send.at[r],
            recv_sem=f_recv.at[r], device_id=partner, device_id_type=MESH,
        ).wait_send()


DMA = pltpu.SemaphoreType.DMA


def body(
    queries, key_rows, value_rows, gate_input, log_decay, head_gain, out_weight, residual,
    mlp_gain, gate_weight, up_weight, down_weight,
):
    freq = np.float32(10000.0 ** -np.linspace(0.0, 1.0, HD // 2))
    freq = jnp.asarray(np.concatenate([freq, freq])[None, :])
    vmem = pl.BlockSpec(memory_space=pltpu.VMEM)
    V = pltpu.VMEM
    return pl.pallas_call(
        kernel,
        out_shape=pltpu.VMEM((QT, D), BF),
        in_specs=[pl.BlockSpec(memory_space=pl.ANY)] * 13,
        out_specs=vmem,
        scratch_shapes=[
            V((TOK, HEADS * HD), BF), V((TOK, HEADS * HD), BF), V((TOK, HEADS * HD), BF), V((TOK, HEADS * HD), BF),
            V((HEADS, TOK), F32), V((1, HD), F32), V((1, HEADS * HD), F32), V((HEADS * HD, D), BF), V((QT, D), BF),
            V((1, D), F32), V((ROWS, FF), BF), V((ROWS, FF), BF), V((ROWS, FF), BF), DMA((13,)),
            V((3, D, FF), BF),
            V((TOK, HD), F32),
            V((TOK, HEADS * HD), BF),
            V((TOK, HEADS * HD), F32),
            V((TOK, HEADS * HD), BF),
            V((8, 80, HD), BF),
            V((8, 80, HD), BF),
            V((8, 64, HD), F32),
            V((64, HD), F32),
            V((80, HD), BF),
            V((8, 80, HD), BF),
            V((8, 64, HD), BF),
            V((8, 64, HD), BF),
            V((TOK, D), BF),
            V((NT - 1, QT, D), BF),
            V((TOK, D), BF),
            V((QT, D), F32),
            V((TOK, FF), F32),
            V((TOK, FF), F32),
            V((TOK, FF), BF),
            V((NZ, TOK, 256), BF),
            V((NT - 1, NZ, QT, 256), BF),
            DMA((3, NZ, NX)),
            DMA((3,)),
            DMA((3, NZ)),
            DMA((3, NZ)),
            DMA((8,)), DMA((8,)), DMA((8,)), DMA((8,)), DMA((8,)), DMA((8,)),
            DMA((NT,)), DMA((NT,)), DMA((NT,)), DMA((NT,)), DMA((NT,)), DMA((NT,)),
        ],
        compiler_params=pltpu.CompilerParams(
            collective_id=0, has_side_effects=True, vmem_limit_bytes=56 * 1024 * 1024
        ),
    )(
        queries, key_rows, value_rows, gate_input, log_decay.T, freq, head_gain[None, :], out_weight, residual,
        mlp_gain[None, :], gate_weight, up_weight, down_weight.T,
    )


def solution(mesh):
    finer = Mesh(mesh.devices.reshape(NZ, NX, NC, NT), ("z", "x", "c", "tp"))
    in_specs = (
        P(SP, "tp"), P(SP, "tp"), P(SP, "tp"), P(SP, "tp"), P(SP, "tp"), P("tp"), P("tp", None),
        P(SP, None), P(), P(SP, "tp"), P(SP, "tp"), P("tp", SP),
    )
    out_specs = P(("z", "x", "c", "tp"), None)
    return jax.shard_map(body, mesh=finer, in_specs=in_specs, out_specs=out_specs, check_vma=False)
```

```python
import heapq

import jax
import jax.numpy as jnp
import numpy as np
from jax import lax
from jax.experimental import pallas as pl
from jax.experimental.pallas import tpu as pltpu
from jax.sharding import Mesh
from jax.sharding import PartitionSpec as P

BF = jnp.bfloat16
F32 = jnp.float32
MESH = pl.DeviceIdType.MESH
HIGH = lax.Precision.HIGHEST
EPS = 1e-06

NZ, NX, NC, NT = 8, 4, 2, 4
SP = ("z", "x", "c")
TOK = 128
HD = 128
HEADS = 4
D = 2048
FF = 1408
ROWS = 32
QT = TOK // NT
GATE, UP, DOWN = 0, 1, 2

PIECE_US = 2.1
HOP_US = 4.0
LEAF_US = 0.5
LEAD = 1.0
LINKS = ("z+", "z-", "x+", "x-")
CODES = (
    16, 241, 6, 271, 144, 113, 134, 15, 272, 225, 246, 267, 32, 97, 118, 127, 160, 22, 11, 377,
    280, 230, 239, 101, 48, 166, 175, 81, 36, 250, 31, 213, 252, 382, 279, 85, 188, 54, 63, 209,
    136, 106, 95, 233, 140, 370, 171, 365, 204, 178, 27, 45, 68, 218, 223, 77, 64, 374, 59, 153,
    180, 194, 203, 109, 292, 90, 75, 349, 120, 158, 151, 357, 284, 186, 199, 41, 308, 338, 347, 333,
    260, 362, 355, 341, 300, 298, 291, 324, 317, 322, 331, 314, 307,
)


def sender_name(key, link):
    a, dz, dx = key
    if link == "z+":
        return (a, (dz - 1) % NZ, dx)
    if link == "z-":
        return (a, (dz + 1) % NZ, dx)
    if link == "x+":
        return (a, dz, (dx - 1) % NX)
    return (a, dz, (dx + 1) % NX)


def exchange_plan():
    onward = {}
    for turn, code in enumerate(CODES):
        key, link = (code // 128, code // 16 % 8, code // 4 % 4), LINKS[code % 4]
        onward.setdefault(sender_name(key, link), []).append((turn, link, key))
    pending = {link: [] for link in LINKS}
    free = dict.fromkeys(LINKS, 0.0)
    arrivals, ops, since = [], [], {}

    def ready(now, key):
        for turn, link, there in onward.get(key, ()):
            since[turn] = now
            heapq.heappush(pending[link], (turn, there))

    for a in (GATE, UP, DOWN):
        ready(0.0, (a, 0, 0))
    now = 0.0
    while True:
        for link, queue in pending.items():
            if queue and free[link] <= now:
                turn, key = heapq.heappop(queue)
                free[link] = now + PIECE_US
                ops.append((max(since[turn], now - LEAD * PIECE_US), 1, "send", link, key))
                heapq.heappush(arrivals, (now + PIECE_US + HOP_US, key))
        if not arrivals:
            break
        now = min([arrivals[0][0]] + [u for link, u in free.items() if pending[link] and u > now])
        while arrivals and arrivals[0][0] <= now + 1e-9:
            _, key = heapq.heappop(arrivals)
            ops.append((now, 0, "recv", None, key))
            ready(now, key)
    due = {}
    for time, _, kind, link, key in ops:
        if kind == "send":
            held = sender_name(key, link)
            due[held] = min(time, due.get(held, time))
    ops = [
        (due.get(key, time + LEAF_US), order, kind, link, key) if kind == "recv" else (time, order, kind, link, key)
        for time, order, kind, link, key in ops
    ]
    ops.sort(key=lambda op: (op[0], op[1]))
    return ops


PLAN = exchange_plan()
SENT = {a: sum(1 for op in PLAN if op[2] == "send" and op[4][0] == a) for a in (GATE, UP, DOWN)}

T_CONTRIB, T_GROUP, T_ALONG, T_BACK, T_SUM1, T_GATHER = 3.0, 11.0, 20.0, 28.0, 37.5, 46.0


def head_cols(h):
    return slice(h * HD, (h + 1) * HD)


def split_log(total):
    hi = total.astype(BF).astype(F32)
    rest = total - hi
    mid = rest.astype(BF).astype(F32)
    low = rest - mid
    i = lax.broadcasted_iota(jnp.int32, (16, HD), 0)
    return jnp.where(i == 0, hi, jnp.where(i == 1, mid, low)).astype(BF)


def join_log(tile):
    t = tile.astype(F32)
    return t[0:1] + t[1:2] + t[2:3]


def silu(v):
    return v * (1.0 / (1.0 + jnp.exp(-v)))


def kernel(
    q_hbm, k_hbm, v_hbm, gi_hbm, ld_hbm, freq_hbm, hg_hbm, ow_hbm, res_hbm, mg_hbm, gw_hbm, uw_hbm, dw_hbm,
    out_ref,
    q_ref, k_ref, v_ref, gi_ref, ld_ref, freq_ref, hg_ref, ow_ref, res_ref, mg_ref, gw_ref, uw_ref, dw_ref, in_sem,
    w, ldp, qrot, inner, ret, stout, stin, pre, came_ref, zout, zin, bout, bin_, po, rs1, nfull, mid,
    gacc, uacc, hid, fo, rs2,
    w_recv, w_send, d_recv, d_send,
    g_recv, g_send, z_recv, z_send, b_recv, b_send, r_recv, r_send, n_recv, n_send, f_recv, f_send,
):
    z, x, c, t = lax.axis_index("z"), lax.axis_index("x"), lax.axis_index("c"), lax.axis_index("tp")
    pos = x * NC + c

    def group_peer(r):
        p = lax.rem(pos + r, NX * NC)
        return p, (z, lax.div(p, NC), lax.rem(p, NC), t)

    def z_peer(r):
        return (lax.rem(z + r, NZ), x, c, t)

    def tp_peer(r):
        j = lax.rem(t + r, NT)
        return j, (z, x, c, j)

    neighbours = {
        "z+": (lax.rem(z + 1, NZ), x, c, t),
        "z-": (lax.rem(z + NZ - 1, NZ), x, c, t),
        "x+": (z, lax.rem(x + 1, NX), c, t),
        "x-": (z, lax.rem(x + NX - 1, NX), c, t),
    }
    partner = (z, x, 1 - c, t)

    mine = pl.ds(pl.multiple_of(t * QT, QT), QT)
    inputs = {
        "gw": (gw_hbm, gw_ref), "uw": (uw_hbm, uw_ref), "dw": (dw_hbm, dw_ref), "freq": (freq_hbm, freq_ref),
        "ld": (ld_hbm, ld_ref), "k": (k_hbm, k_ref), "v": (v_hbm, v_ref), "q": (q_hbm, q_ref),
        "gi": (gi_hbm, gi_ref), "hg": (hg_hbm, hg_ref), "ow": (ow_hbm, ow_ref),
        "res": (res_hbm.at[mine, :], res_ref), "mg": (mg_hbm, mg_ref),
    }
    loads = {
        name: pltpu.make_async_copy(src, dst, in_sem.at[i]) for i, (name, (src, dst)) in enumerate(inputs.items())
    }
    for load in loads.values():
        load.start()

    def loaded(*names):
        for name in names:
            loads[name].wait()

    barrier = pltpu.get_barrier_semaphore()
    for r in range(1, NX * NC):
        pl.semaphore_signal(barrier, inc=1, device_id=group_peer(r)[1], device_id_type=MESH)
    for r in range(1, NZ):
        pl.semaphore_signal(barrier, inc=1, device_id=z_peer(r), device_id_type=MESH)
    for r in range(1, NT):
        pl.semaphore_signal(barrier, inc=1, device_id=tp_peer(r)[1], device_id_type=MESH)
    loaded("gw", "uw", "dw")
    pl.semaphore_wait(barrier, NX * NC - 1 + NZ - 1 + NT - 1)

    own = {GATE: gw_ref, UP: uw_ref, DOWN: dw_ref}

    def rows_of(dz, dx, core):
        sz = lax.rem(z + NZ - dz, NZ)
        sx = lax.rem(x + NX - dx, NX)
        return pl.ds(pl.multiple_of(((sz * NX + sx) * NC + core) * ROWS, ROWS), ROWS)

    def at_home(key):
        a, dz, dx = key
        return w.at[a, rows_of(dz, dx, c), :]

    def source(key):
        return own[key[0]] if key[1:] == (0, 0) else at_home(key)

    def hop(link, key):
        a, dz, dx = key
        held = sender_name(key, link)
        return pltpu.make_async_remote_copy(
            src_ref=source(held), dst_ref=at_home(held), send_sem=w_send.at[a],
            recv_sem=w_recv.at[a, dz, dx], device_id=neighbours[link], device_id_type=MESH,
        )

    def across(key):
        a, dz, dx = key
        return pltpu.make_async_remote_copy(
            src_ref=source(key), dst_ref=at_home(key), send_sem=d_send.at[a, dz],
            recv_sem=d_recv.at[a, dz], device_id=partner, device_id_type=MESH,
        )

    cursor = [0]

    def step(op):
        _, _, kind, link, key = op
        if kind == "send":
            hop(link, key).start()
        else:
            a, dz, dx = key
            pltpu.make_async_remote_copy(
                src_ref=at_home(key), dst_ref=at_home(key), send_sem=w_send.at[a],
                recv_sem=w_recv.at[a, dz, dx], device_id=partner, device_id_type=MESH,
            ).wait_recv()
            across(key).start()

    def run_until(time):
        while cursor[0] < len(PLAN) and PLAN[cursor[0]][0] <= time:
            step(PLAN[cursor[0]])
            cursor[0] += 1

    def run_until_received(wanted):
        last = max(i for i, op in enumerate(PLAN) if op[2] == "recv" and wanted(op[4]))
        while cursor[0] <= last:
            step(PLAN[cursor[0]])
            cursor[0] += 1

    def wait_across(a, dz):
        whole = w.at[a, pl.ds(0, NX * ROWS), :]
        pltpu.make_async_remote_copy(
            src_ref=whole, dst_ref=whole, send_sem=d_send.at[a, dz],
            recv_sem=d_recv.at[a, dz], device_id=partner, device_id_type=MESH,
        ).wait_recv()

    run_until(0.0)
    for a in (GATE, UP, DOWN):
        across((a, 0, 0)).start()

    loaded("freq")
    row = lax.broadcasted_iota(jnp.int32, (TOK, HD), 0) + ((z * NX + x) * NC + c) * TOK
    angles = row.astype(F32) * freq_ref[...]
    cosv = jnp.cos(angles)
    sinv = jnp.sin(angles)
    sinv = jnp.where(lax.broadcasted_iota(jnp.int32, (TOK, HD), 1) < HD // 2, -sinv, sinv)
    loaded("ld", "k", "v")
    ldp[...] = jnp.zeros((TOK, HD), F32)
    ldp[0:HEADS, :] = ld_ref[...]
    ti = lax.broadcasted_iota(jnp.int32, (TOK, TOK), 0)
    si = lax.broadcasted_iota(jnp.int32, (TOK, TOK), 1)
    lower = si <= ti
    cum_t = jnp.dot(ldp[...], (ti <= si).astype(F32), precision=HIGH, preferred_element_type=F32)
    cum = cum_t.T
    krots = []
    for h in range(HEADS):
        kf = k_ref[:, head_cols(h)].astype(F32)
        krot = ((kf * cosv + pltpu.roll(kf, HD // 2, 1) * sinv) * HD ** (-0.5)).astype(BF)
        krots.append(krot)
        col = cum[:, h : h + 1]
        last = cum[TOK - 1 : TOK, h : h + 1]
        kw = (krot.astype(F32) * jnp.exp(last - col)).astype(BF)
        contrib = jnp.dot(kw.T, v_ref[:, head_cols(h)], preferred_element_type=F32)
        logs = split_log(jnp.broadcast_to(last, (1, HD)))
        for half in range(2):
            stout[2 * h + half, 0:64, :] = contrib[64 * half : 64 * half + 64].astype(BF)
            stout[2 * h + half, 64:80, :] = logs
    for a in (GATE, UP, DOWN):
        w[a, rows_of(0, 0, c), :] = own[a][...]
    run_until(T_CONTRIB)

    def group_copy(r):
        p, peer = group_peer(r)
        return pltpu.make_async_remote_copy(
            src_ref=stout.at[p], dst_ref=stin.at[pos], send_sem=g_send.at[r],
            recv_sem=g_recv.at[r], device_id=peer, device_id_type=MESH,
        )

    for r in range(1, NX * NC):
        group_copy(r).start()
    stin[pos] = stout[pos]

    loaded("q")
    for h in range(HEADS):
        qf = q_ref[:, head_cols(h)].astype(F32)
        qr = (qf * cosv + pltpu.roll(qf, HD // 2, 1) * sinv).astype(BF)
        qrot[:, head_cols(h)] = qr
        spread = cum[:, h : h + 1] - cum_t[h : h + 1, :]
        weight = jnp.where(lower, jnp.exp(jnp.where(lower, spread, 0.0)), 0.0)
        scores = lax.dot_general(qr, krots[h], (((1,), (1,)), ((), ())), preferred_element_type=F32)
        probs = (scores * weight).astype(BF)
        inner[:, head_cols(h)] = jnp.dot(probs, v_ref[:, head_cols(h)], preferred_element_type=F32)
    run_until(T_GROUP)

    for r in range(1, NX * NC):
        group_copy(r).wait_recv()
    run = jnp.zeros((64, HD), F32)
    sofar = jnp.zeros((1, HD), F32)
    reach = []
    for p in range(NX * NC):
        pre[p] = run
        reach.append(sofar)
        log = join_log(stin[p, 64:80, :])
        run = run * jnp.exp(log) + stin[p, 0:64, :].astype(F32)
        sofar = sofar + log
    zout[0:64, :] = run.astype(BF)
    zout[64:80, :] = split_log(sofar)

    def z_copy(r):
        return pltpu.make_async_remote_copy(
            src_ref=zout, dst_ref=zin.at[z], send_sem=z_send.at[r],
            recv_sem=z_recv.at[r], device_id=z_peer(r), device_id_type=MESH,
        )

    for r in range(1, NZ):
        @pl.when(z + r < NZ)
        def _():
            z_copy(r).start()
    run_until(T_ALONG)
    for r in range(1, NZ):
        @pl.when(z >= r)
        def _():
            z_copy(r).wait_recv()
    came_ref[...] = jnp.zeros((64, HD), F32)
    for s in range(NZ - 1):
        @pl.when(s < z)
        def _():
            decay = jnp.exp(join_log(zin[s, 64:80, :]))
            came_ref[...] = came_ref[...] * decay + zin[s, 0:64, :].astype(F32)
    came = came_ref[...]
    for p in range(NX * NC):
        bout[p] = (pre[p] + jnp.exp(reach[p]) * came).astype(BF)

    def back_copy(r):
        p, peer = group_peer(r)
        return pltpu.make_async_remote_copy(
            src_ref=bout.at[p], dst_ref=bin_.at[pos], send_sem=b_send.at[r],
            recv_sem=b_recv.at[r], device_id=peer, device_id_type=MESH,
        )

    for r in range(1, NX * NC):
        back_copy(r).start()
    bin_[pos] = bout[pos]
    run_until(T_BACK)
    for r in range(1, NX * NC):
        back_copy(r).wait_recv()

    loaded("gi", "hg", "ow", "res", "mg")
    for h in range(HEADS):
        before = bin_[2 * h : 2 * h + 2].reshape(HD, HD)
        cross = jnp.dot(qrot[:, head_cols(h)], before, preferred_element_type=F32)
        res = inner[:, head_cols(h)] + cross * jnp.exp(cum[:, h : h + 1])
        scale = lax.rsqrt(jnp.mean(res * res, axis=-1, keepdims=True) + EPS)
        gain = hg_ref[:, head_cols(h)]
        ret[:, head_cols(h)] = (
            res * scale * gain * silu(gi_ref[:, head_cols(h)].astype(F32))
        ).astype(BF)
    for n in range(0, D, 512):
        po[:, n : n + 512] = jnp.dot(
            ret[...], ow_ref[:, n : n + 512], preferred_element_type=F32
        ).astype(BF)

    def sum_copy(r):
        j, peer = tp_peer(r)
        return pltpu.make_async_remote_copy(
            src_ref=po.at[pl.ds(pl.multiple_of(j * QT, QT), QT), :], dst_ref=rs1.at[r - 1],
            send_sem=r_send.at[r], recv_sem=r_recv.at[r], device_id=peer, device_id_type=MESH,
        )

    for r in (2, 1, 3):
        sum_copy(r).start()
    run_until(T_SUM1)
    for r in range(1, NT):
        sum_copy(r).wait_recv()
    mixed = po[mine, :].astype(F32)
    for r in range(NT - 1):
        mixed = mixed + rs1[r].astype(F32)
    middle = (res_ref[...].astype(F32) + mixed).astype(BF).astype(F32)
    mid[...] = middle
    scale = lax.rsqrt(jnp.mean(middle * middle, axis=-1, keepdims=True) + EPS)
    nfull[mine, :] = (middle * scale * mg_ref[...]).astype(BF)

    def norm_copy(r):
        return pltpu.make_async_remote_copy(
            src_ref=nfull.at[mine, :], dst_ref=nfull.at[mine, :],
            send_sem=n_send.at[r], recv_sem=n_recv.at[r], device_id=tp_peer(r)[1],
            device_id_type=MESH,
        )

    def norm_arrived(r):
        rows = nfull.at[pl.ds(pl.multiple_of(lax.rem(t + NT - r, NT) * QT, QT), QT), :]
        pltpu.make_async_remote_copy(
            src_ref=rows, dst_ref=rows, send_sem=n_send.at[r], recv_sem=n_recv.at[r],
            device_id=partner, device_id_type=MESH,
        ).wait_recv()

    for r in (2, 1, 3):
        norm_copy(r).start()
    run_until(T_GATHER)
    for r in range(1, NT):
        norm_arrived(r)

    run_until_received(lambda key: key[0] != DOWN)
    for a in (GATE, UP):
        for dz in range(NZ):
            wait_across(a, dz)
    clock = PLAN[cursor[0] - 1][0]
    for n in range(NZ):
        rows = slice(n * 256, (n + 1) * 256)
        for a, acc in ((GATE, gacc), (UP, uacc)):
            term = jnp.dot(nfull[:, rows], w[a, rows, :], preferred_element_type=F32)
            acc[...] = term if n == 0 else acc[...] + term
        clock += 0.6
        run_until(clock)
    hid[...] = (silu(gacc[...]) * uacc[...]).astype(BF)

    def ffn_copy(r, zc):
        j, peer = tp_peer(r)
        return pltpu.make_async_remote_copy(
            src_ref=fo.at[zc, pl.ds(pl.multiple_of(j * QT, QT), QT), :], dst_ref=rs2.at[r - 1, zc],
            send_sem=f_send.at[r], recv_sem=f_recv.at[r], device_id=peer, device_id_type=MESH,
        )

    last = {}
    for i, op in enumerate(PLAN):
        if op[2] == "recv" and op[4][0] == DOWN:
            last[op[4][1]] = i
    for dz in sorted(range(NZ), key=lambda k: last[k]):
        run_until_received(lambda key: key[0] == DOWN and key[1] == dz)
        wait_across(DOWN, dz)
        zc = lax.rem(z + NZ - dz, NZ)
        rows = pl.ds(pl.multiple_of(zc * 256, 256), 256)
        fo[zc] = lax.dot_general(
            hid[...], w[DOWN, rows, :], (((1,), (1,)), ((), ())), preferred_element_type=F32
        ).astype(BF)
        for r in (2, 1, 3):
            ffn_copy(r, zc).start()
    run_until(1e9)
    for r in range(1, NT):
        pltpu.make_async_remote_copy(
            src_ref=rs2.at[r - 1], dst_ref=rs2.at[r - 1], send_sem=f_send.at[r],
            recv_sem=f_recv.at[r], device_id=partner, device_id_type=MESH,
        ).wait_recv()
    for n in range(NZ):
        cols = slice(n * 256, (n + 1) * 256)
        total = fo[n, mine, :].astype(F32)
        for r in range(NT - 1):
            total = total + rs2[r, n].astype(F32)
        out_ref[:, cols] = (mid[:, cols] + total).astype(BF)

    for a in (GATE, UP, DOWN):
        sent = w.at[a, pl.ds(0, SENT[a] * ROWS), :]
        pltpu.make_async_remote_copy(
            src_ref=sent, dst_ref=sent, send_sem=w_send.at[a], recv_sem=w_recv.at[a, 0, 0],
            device_id=partner, device_id_type=MESH,
        ).wait_send()
        for dz in range(NZ):
            whole = w.at[a, pl.ds(0, NX * ROWS), :]
            pltpu.make_async_remote_copy(
                src_ref=whole, dst_ref=whole, send_sem=d_send.at[a, dz],
                recv_sem=d_recv.at[a, dz], device_id=partner, device_id_type=MESH,
            ).wait_send()
    for r in range(1, NX * NC):
        group_copy(r).wait_send()
        back_copy(r).wait_send()
    for r in range(1, NZ):
        @pl.when(z + r < NZ)
        def _():
            z_copy(r).wait_send()
    for r in range(1, NT):
        sum_copy(r).wait_send()
        norm_copy(r).wait_send()
        pltpu.make_async_remote_copy(
            src_ref=rs2.at[r - 1], dst_ref=rs2.at[r - 1], send_sem=f_send.at[r],
            recv_sem=f_recv.at[r], device_id=partner, device_id_type=MESH,
        ).wait_send()


DMA = pltpu.SemaphoreType.DMA


def body(
    queries, key_rows, value_rows, gate_input, log_decay, head_gain, out_weight, residual,
    mlp_gain, gate_weight, up_weight, down_weight,
):
    freq = np.float32(10000.0 ** -np.linspace(0.0, 1.0, HD // 2))
    freq = jnp.asarray(np.concatenate([freq, freq])[None, :])
    vmem = pl.BlockSpec(memory_space=pltpu.VMEM)
    V = pltpu.VMEM
    return pl.pallas_call(
        kernel,
        out_shape=pltpu.VMEM((QT, D), BF),
        in_specs=[pl.BlockSpec(memory_space=pl.ANY)] * 13,
        out_specs=vmem,
        scratch_shapes=[
            V((TOK, HEADS * HD), BF), V((TOK, HEADS * HD), BF), V((TOK, HEADS * HD), BF), V((TOK, HEADS * HD), BF),
            V((HEADS, TOK), F32), V((1, HD), F32), V((1, HEADS * HD), F32), V((HEADS * HD, D), BF), V((QT, D), BF),
            V((1, D), F32), V((ROWS, FF), BF), V((ROWS, FF), BF), V((ROWS, FF), BF), DMA((13,)),
            V((3, D, FF), BF),
            V((TOK, HD), F32),
            V((TOK, HEADS * HD), BF),
            V((TOK, HEADS * HD), F32),
            V((TOK, HEADS * HD), BF),
            V((8, 80, HD), BF),
            V((8, 80, HD), BF),
            V((8, 64, HD), F32),
            V((64, HD), F32),
            V((80, HD), BF),
            V((8, 80, HD), BF),
            V((8, 64, HD), BF),
            V((8, 64, HD), BF),
            V((TOK, D), BF),
            V((NT - 1, QT, D), BF),
            V((TOK, D), BF),
            V((QT, D), F32),
            V((TOK, FF), F32),
            V((TOK, FF), F32),
            V((TOK, FF), BF),
            V((NZ, TOK, 256), BF),
            V((NT - 1, NZ, QT, 256), BF),
            DMA((3, NZ, NX)),
            DMA((3,)),
            DMA((3, NZ)),
            DMA((3, NZ)),
            DMA((8,)), DMA((8,)), DMA((8,)), DMA((8,)), DMA((8,)), DMA((8,)),
            DMA((NT,)), DMA((NT,)), DMA((NT,)), DMA((NT,)), DMA((NT,)), DMA((NT,)),
        ],
        compiler_params=pltpu.CompilerParams(
            collective_id=0, has_side_effects=True, vmem_limit_bytes=56 * 1024 * 1024
        ),
    )(
        queries, key_rows, value_rows, gate_input, log_decay.T, freq, head_gain[None, :], out_weight, residual,
        mlp_gain[None, :], gate_weight, up_weight, down_weight.T,
    )


def solution(mesh):
    finer = Mesh(mesh.devices.reshape(NZ, NX, NC, NT), ("z", "x", "c", "tp"))
    in_specs = (
        P(SP, "tp"), P(SP, "tp"), P(SP, "tp"), P(SP, "tp"), P(SP, "tp"), P("tp"), P("tp", None),
        P(SP, None), P(), P(SP, "tp"), P(SP, "tp"), P("tp", SP),
    )
    out_specs = P(("z", "x", "c", "tp"), None)
    return jax.shard_map(body, mesh=finer, in_specs=in_specs, out_specs=out_specs, check_vma=False)
```
